32 devices in a mesh: sp: 4 (over z), fs: 4 (over y, x), tp: 2 (over core).
Axes of the slice: x: 2, y: 2, z: 4, core: 2. Of those that a mesh axis runs over, the one named last changes fastest.
Arguments:
- tokens: bfloat16 [4, 1024, 2048], P('fs', 'sp', 'tp'), may hold values from -6 to 6
- norm_gain: float32 [2048], replicated, may hold values from 0.1 to 1.9
- query_weight: bfloat16 [2048, 1024], P(('sp', 'fs'), 'tp'), may hold values from -0.125 to 0.125
- forget_weight: bfloat16 [2048, 1024], P(('sp', 'fs'), 'tp'), may hold values from -0.125 to 0.125
- value_weight: bfloat16 [2048, 1024], P(('sp', 'fs'), 'tp'), may hold values from -0.125 to 0.125
- outgate_weight: bfloat16 [2048, 1024], P(('sp', 'fs'), 'tp'), may hold values from -0.125 to 0.125
- pool_in_weight: bfloat16 [2048, 1024], P(('sp', 'fs'), 'tp'), may hold values from -0.125 to 0.125
- forget_room: float32 [1024], P('tp'), may hold values from 0 to 0.06
- decay_shift: float32 [4, 1024, 8], P('fs', 'sp', 'tp'), may hold values from -0.6 to 0
- head_gain: float32 [128], replicated, may hold values from 0.1 to 1.9
- start_state: float32 [4, 8, 128, 128], P('fs', 'tp'), may hold values from -0.09375 to 0.09375
- pool_map: bfloat16 [4, 256, 256], P('tp'), may hold values from -0.375 to 0.375
- pool_scale: float32 [1024], P('tp'), may hold values from 0.1 to 1.9
- out_rec_weight: bfloat16 [1024, 2048], P('tp', ('sp', 'fs')), may hold values from -0.125 to 0.125
- out_pool_weight: bfloat16 [1024, 2048], P('tp', ('sp', 'fs')), may hold values from -0.125 to 0.125
Outputs:
- mixed: bfloat16 [4, 1024, 2048], P('fs', ('sp', 'tp'))
The draws below stay inside these ranges and needn't reach their ends.
All inputs are finite; a program needn't handle non-finite values.
Results may differ from the reference program's by a relative error of at most 0.013.
Values may be sent and summed in bfloat16 or wider, within the bound.
No kernel may reach another device: no remote copies, remote signals or barrier semaphores. Data moves between devices by JAX's collectives and lax.ppermute only.
A program may use at most 128 MiB of HBM per device.

```python
import jax
import jax.numpy as jnp
from jax import lax

D = 2048
REC_HEADS = 8
HEAD = 128
POOL_GROUPS = 4
POOL_DIM = 256
D_REC = 1024
D_POOL = 1024
WIDEST = 16
TOK_DEV = 256
BLOCK = 128
STREAM_EXTENT = 1024
SEQUENCE_COUNT = 4
N_TP = 2


def fast_heads(key):
    uniforms = jax.random.uniform(jax.random.fold_in(key, 11), (REC_HEADS,))
    return uniforms < 0.5


def draw_forget_room(key, part):
    fast_mask = fast_heads(key)
    spread = jax.random.uniform(jax.random.fold_in(key, 1), (REC_HEADS, HEAD))
    slow_room = 0.3 * jnp.exp(spread * jnp.log(4.0)) / STREAM_EXTENT
    fast_room = 0.02 * jnp.exp(spread * jnp.log(3.0))
    return jnp.where(fast_mask[:, None], fast_room, slow_room).reshape(REC_HEADS * HEAD).astype(jnp.float32)


def draw_decay_shift(key, part):
    fast_mask = fast_heads(key)
    device_blocks = STREAM_EXTENT // TOK_DEV
    spread = jax.random.uniform(jax.random.fold_in(key, 2), (SEQUENCE_COUNT, device_blocks, REC_HEADS))
    factor = jnp.exp(spread * jnp.log(4.0))
    fading_rate = jnp.where(fast_mask[None, None, :], 0.005 * factor, 0.15 * factor / STREAM_EXTENT)
    fading_rate = jnp.repeat(fading_rate, TOK_DEV, axis=1)
    pulse_locations = jax.random.randint(jax.random.fold_in(key, 3), (SEQUENCE_COUNT, 2), 0, STREAM_EXTENT)
    criterion_parts = jnp.log(0.6 + 0.2 * jax.random.uniform(jax.random.fold_in(key, 4), (SEQUENCE_COUNT, 2, REC_HEADS)))
    pulse_consensus = (jnp.arange(STREAM_EXTENT)[None, :, None] == pulse_locations[:, None, :]).astype(jnp.float32)
    pulse_markers = jnp.einsum('ydw,ywu->ydu', pulse_consensus, criterion_parts)
    return (pulse_markers - fading_rate).astype(jnp.float32)


def block_scale(rng, shape, pieces, smallest, high):
    level = 1.0
    for dim, shards_of in pieces:
        draws = jax.random.uniform(jax.random.fold_in(jax.random.fold_in(rng, 6), dim), (shards_of,), jnp.float32, smallest / len(pieces), high / len(pieces))
        level = level * jnp.repeat(jnp.exp(draws), shape[dim] // shards_of).reshape((-1,) + (1,) * (len(shape) - 1 - dim))
    return level


def noise(key, dims, deviation, most, pieces=(), held_as=jnp.bfloat16):
    values = deviation * jax.random.normal(key, dims, jnp.float32)
    if pieces:
        values = values * block_scale(key, dims, pieces, -0.22, 0.18)
    return jnp.clip(values, -most, most).astype(held_as)


def setup_inputs(seed: int = 0) -> dict:
    arg_keys = jax.random.split(jax.random.key(seed), 16)
    return {
        "tokens": noise(arg_keys[0], (SEQUENCE_COUNT, STREAM_EXTENT, D), 1.0, 6.0, ((0, 4), (1, 4), (2, 2))),
        "norm_gain": jnp.clip(1.0 + 0.18 * jax.random.normal(arg_keys[1], (D,), jnp.float32), 0.1, 1.9),
        "query_weight": noise(arg_keys[2], (D, D_REC), D ** -0.5, 0.125, ((0, 16), (1, 2))),
        "forget_weight": noise(arg_keys[3], (D, D_REC), D ** -0.5, 0.125, ((0, 16), (1, 2))),
        "value_weight": noise(arg_keys[4], (D, D_REC), D ** -0.5, 0.125, ((0, 16), (1, 2))),
        "outgate_weight": noise(arg_keys[5], (D, D_REC), D ** -0.5, 0.125, ((0, 16), (1, 2))),
        "pool_in_weight": noise(arg_keys[6], (D, D_POOL), D ** -0.5, 0.125, ((0, 16), (1, 2))),
        "forget_room": draw_forget_room(jax.random.fold_in(arg_keys[15], 71), 0),
        "decay_shift": draw_decay_shift(jax.random.fold_in(arg_keys[15], 71), 0),
        "head_gain": jnp.clip(1.0 + 0.18 * jax.random.normal(arg_keys[9], (HEAD,), jnp.float32), 0.1, 1.9),
        "start_state": noise(arg_keys[10], (SEQUENCE_COUNT, REC_HEADS, HEAD, HEAD), (0.5 * STREAM_EXTENT ** -0.5), 0.09375, ((0, 4), (1, 2)), jnp.float32),
        "pool_map": noise(arg_keys[11], (POOL_GROUPS, POOL_DIM, POOL_DIM), POOL_DIM ** -0.5, 0.375, ((0, 2),)),
        "pool_scale": jnp.clip(1.0 + 0.18 * jax.random.normal(arg_keys[12], (D_POOL,), jnp.float32), 0.1, 1.9),
        "out_rec_weight": noise(arg_keys[13], (D_REC, D), (D_REC + D_POOL) ** -0.5, 0.125, ((0, 2), (1, 16))),
        "out_pool_weight": noise(arg_keys[14], (D_POOL, D), (D_REC + D_POOL) ** -0.5, 0.125, ((0, 2), (1, 16))),
    }


EPSILON = 1e-06

def rms_scale(entry_vectors):
    return lax.rsqrt(lax.optimization_barrier(jnp.mean(entry_vectors * entry_vectors, axis=-1, keepdims=True)) + EPSILON)

def rounded(entry_vectors):
    return lax.optimization_barrier(entry_vectors.astype(jnp.bfloat16)).astype(jnp.float32)

def recurrence(query_rows, forget_logits, value_rows, outgate, forget_room, lagged_tokens, head_gain, memory_start):
    length = query_rows.shape[0]
    head_count = query_rows.shape[1] // HEAD
    blocks = length // BLOCK
    queries = jax.nn.silu(query_rows.astype(jnp.float32)) * HEAD ** (-0.5)
    keyed = forget_room[None, :] * (1.0 - jax.nn.sigmoid(forget_logits.astype(jnp.float32)))
    log_decay = jnp.log1p(-keyed).reshape(length, head_count, HEAD) + lagged_tokens[:, :, None]

    def to_blocks(entry_vectors):
        return entry_vectors.reshape(blocks, BLOCK, head_count, HEAD).transpose(0, 2, 1, 3)
    causal = jnp.tril(jnp.ones((BLOCK, BLOCK), jnp.float32))

    def advance(memory, inputs):
        query_block, key_block, value_block, decay_block = inputs
        within = jnp.cumsum(decay_block, axis=1)
        centre = within[:, BLOCK // 2 - 1:BLOCK // 2]
        ending = within[:, BLOCK - 1:BLOCK]
        scores = jnp.einsum('hcd,hsd->hcs', rounded(query_block * jnp.exp(within - centre)), rounded(key_block * jnp.exp(centre - within))) * causal
        inside = jnp.einsum('hcs,hse->hce', rounded(scores), value_block)
        carried = jnp.einsum('hcd,hde->hce', rounded(query_block * jnp.exp(within)), rounded(memory))
        added = jnp.einsum('hcd,hce->hde', rounded(key_block * jnp.exp(ending - within)), value_block)
        memory = jnp.exp(ending[:, 0, :])[:, :, None] * memory + added
        return (memory, inside + carried)
    inputs = (to_blocks(queries), to_blocks(keyed), to_blocks(value_rows.astype(jnp.float32)), to_blocks(log_decay.reshape(length, head_count * HEAD)))
    _, outputs = lax.scan(advance, memory_start, inputs)
    outputs = outputs.transpose(0, 2, 1, 3).reshape(length, head_count, HEAD)
    gating = jax.nn.silu(outgate.astype(jnp.float32)).reshape(length, head_count, HEAD)
    result = outputs * rms_scale(outputs) * head_gain * gating
    return result.reshape(length, head_count * HEAD).astype(jnp.bfloat16)

def pooling(pool_input, pool_map, pool_scale):
    length = pool_input.shape[0]
    columns = pool_input.shape[1]
    entry_vectors = pool_input.astype(jnp.float32)
    front_filled = jnp.concatenate([jnp.zeros((WIDEST, columns), jnp.float32), entry_vectors], axis=0)
    group_index = (jnp.arange(columns, dtype=jnp.int32) // POOL_DIM).astype(jnp.int32)
    reach = jnp.left_shift(jnp.int32(2), group_index)
    window_sum = jnp.zeros((length, columns), jnp.float32)
    for offset in range(WIDEST):
        window_sum = window_sum + front_filled[WIDEST - offset:WIDEST - offset + length] * (offset < reach).astype(jnp.float32)
    position = jnp.arange(length, dtype=jnp.int32)
    amount = jnp.minimum(position[:, None] + 1, reach[None, :]).astype(jnp.float32)
    pooled = (window_sum / amount - entry_vectors).astype(jnp.bfloat16)
    mapped = jnp.einsum('tgc,gcd->tgd', pooled.reshape(length, POOL_GROUPS, POOL_DIM).astype(jnp.float32), pool_map.astype(jnp.float32))
    return (mapped.reshape(length, columns) * pool_scale).astype(jnp.bfloat16)

def reference(tokens, norm_gain, query_weight, forget_weight, value_weight, outgate_weight, pool_in_weight, forget_room, decay_shift, head_gain, start_state, pool_map, pool_scale, out_rec_weight, out_pool_weight):
    rec_part = D_REC // N_TP
    pool_part = D_POOL // N_TP

    def one_sequence(inputs):
        token_rows, lagged_tokens, memory_start = inputs
        widened = token_rows.astype(jnp.float32)
        rescaled_input = (widened * rms_scale(widened) * norm_gain).astype(jnp.bfloat16)
        projected = [jnp.dot(rescaled_input, weight, preferred_element_type=jnp.float32).astype(jnp.bfloat16) for weight in (query_weight, forget_weight, value_weight, outgate_weight, pool_in_weight)]
        rec_out = recurrence(projected[0], projected[1], projected[2], projected[3], forget_room, lagged_tokens, head_gain, memory_start)
        pool_out = pooling(projected[4], pool_map, pool_scale)
        summed = jnp.zeros((token_rows.shape[0], D), jnp.float32)
        for device_part in range(N_TP):
            partial_rows = jnp.dot(rec_out[:, device_part * rec_part:(device_part + 1) * rec_part], out_rec_weight[device_part * rec_part:(device_part + 1) * rec_part], preferred_element_type=jnp.float32)
            partial_rows = partial_rows + jnp.dot(pool_out[:, device_part * pool_part:(device_part + 1) * pool_part], out_pool_weight[device_part * pool_part:(device_part + 1) * pool_part], preferred_element_type=jnp.float32)
            summed = summed + partial_rows.astype(jnp.bfloat16).astype(jnp.float32)
        return summed.astype(jnp.bfloat16)
    return lax.map(one_sequence, (tokens, decay_shift, start_state))
```

```python
import functools

import jax
import jax.numpy as jnp
from jax import lax
from jax.experimental import pallas as pl
from jax.experimental.pallas import tpu as pltpu
from jax.sharding import PartitionSpec as P

HEAD = 128
POOL_DIM = 256
WIDEST = 16
BLOCK = 128
PAIR = 2
EPSILON = 1e-06
F32 = jnp.float32
BF16 = jnp.bfloat16


def dot(a, b, contract):
    return lax.dot_general(a, b, (contract, ((), ())), preferred_element_type=F32)


def swapped(value, axis, distance):
    count = lax.axis_size(axis)
    return lax.ppermute(value, axis, [(i, i ^ distance) for i in range(count)])


def passed_on(value, axis, steps):
    count = lax.axis_size(axis)
    return lax.ppermute(value, axis, [(i, i + steps) for i in range(count - steps)])


def call(kernel, outs, *args, scratch=(), name=None):
    vmem = pl.BlockSpec(memory_space=pltpu.VMEM)
    return pl.pallas_call(
        kernel,
        out_shape=[jax.ShapeDtypeStruct(shape, dtype) for shape, dtype in outs],
        in_specs=[vmem] * len(args),
        out_specs=[vmem] * len(outs),
        scratch_shapes=list(scratch),
        compiler_params=pltpu.CompilerParams(vmem_limit_bytes=50 * 2**20),
        name=name,
    )(*args)


def spread(same, other, groups):
    n_sp, n_fs = lax.axis_size("sp"), lax.axis_size("fs")
    rows = same.shape[0]
    arrived = [same] + [swapped(other if d % PAIR else same, "sp", d) for d in range(1, n_sp)]
    pieces = []
    for group in groups:
        plane = arrived[group[0]] if len(group) == 1 else jnp.concatenate([arrived[d] for d in group], axis=0)
        pieces.append((plane, 0, tuple(group)))
        if n_fs == 4:
            near = [swapped(plane, "fs", 1), swapped(plane, "fs", 2)]
            pieces.append((near[0], 1, tuple(group)))
            pieces.append((near[1], 2, tuple(group)))
            first = [d for d in group if d < n_sp // 2]
            cut = len(first) * rows
            if first:
                pieces.append((swapped(near[1][:cut], "fs", 1), 3, tuple(first)))
            if len(first) < len(group):
                pieces.append((swapped(near[0][cut:], "fs", 2), 3, tuple(group[len(first) :])))
        else:
            for distance in range(1, n_fs):
                pieces.append((swapped(plane, "fs", distance), distance, tuple(group)))
    return pieces


def assemble(refs, where, whole, rows):
    sp, fs, n_fs = lax.axis_index("sp"), lax.axis_index("fs"), lax.axis_size("fs")
    for ref, (c, distances) in zip(refs, where):
        for k, d in enumerate(distances):
            spot = ((sp ^ d) * n_fs + (fs ^ c)) * rows
            whole[pl.ds(pl.multiple_of(spot, rows), rows), :] = ref[k * rows : (k + 1) * rows, :]


def norm_kernel(mine, near, mine_other, near_other, gain, out):
    part, tp = lax.axis_index("sp") % PAIR, lax.axis_index("tp")
    length, width = mine.shape
    here = pl.multiple_of(tp * width, width)
    there = pl.multiple_of((1 - tp) * width, width)
    for spot, left, right in ((part, mine, mine_other), (1 - part, near, near_other)):
        rows = pl.ds(pl.multiple_of(spot * length, length), length)
        a, b = left[...].astype(F32), right[...].astype(F32)
        total = jnp.sum(a * a, axis=1, keepdims=True) + jnp.sum(b * b, axis=1, keepdims=True)
        scale = lax.rsqrt(total / (2 * width) + EPSILON)
        out[rows, pl.ds(here, width)] = (a * scale * gain[:, pl.ds(here, width)]).astype(BF16)
        out[rows, pl.ds(there, width)] = (b * scale * gain[:, pl.ds(there, width)]).astype(BF16)


def cumulative(ones_below, value):
    high = value.astype(BF16)
    rest = value - high.astype(F32)
    middle = rest.astype(BF16)
    low = (rest - middle.astype(F32)).astype(BF16)
    contract = ((1,), (0,))
    return dot(ones_below, high, contract) + (dot(ones_below, middle, contract) + dot(ones_below, low, contract))


def mix_kernel(*refs, where, rows):
    normed, room, shift = refs[:3]
    shards = refs[3 : 3 + len(where)]
    inside_out, reach_out, state_out, fade_out, total_out, last_out, whole = refs[3 + len(where) :]
    assemble(shards, where, whole, rows)
    width = room.shape[1]
    length = normed.shape[0]
    heads = width // HEAD
    projected = dot(normed[...], whole[...], ((1,), (0,))).astype(BF16)
    t = lax.broadcasted_iota(jnp.int32, (BLOCK, BLOCK), 0)
    s = lax.broadcasted_iota(jnp.int32, (BLOCK, BLOCK), 1)
    causal = s <= t
    ones_below = causal.astype(F32).astype(BF16)
    state = [jnp.zeros((HEAD, HEAD), F32) for _ in range(heads)]
    faded = [jnp.zeros((1, HEAD), F32) for _ in range(heads)]
    for n in range(length // BLOCK):
        span = slice(n * BLOCK, (n + 1) * BLOCK)
        logits = projected[span, 0:width].astype(F32)
        query = projected[span, width : 2 * width].astype(F32)
        value = projected[span, 2 * width :]
        keyed = room[...] * (1.0 - jax.nn.sigmoid(logits))
        lag = jnp.concatenate(
            [jnp.broadcast_to(shift[span, h : h + 1], (BLOCK, HEAD)) for h in range(heads)], axis=1
        )
        within = cumulative(ones_below, jnp.log1p(-keyed) + lag)
        queries = jax.nn.silu(query) * HEAD ** (-0.5)
        centre = within[BLOCK // 2 - 1 : BLOCK // 2]
        ending = within[BLOCK - 1 : BLOCK]
        near_q = (queries * jnp.exp(within - centre)).astype(BF16)
        near_k = (keyed * jnp.exp(centre - within)).astype(BF16)
        late_k = (keyed * jnp.exp(ending - within)).astype(BF16)
        reach_out[span, :] = (queries * jnp.exp(within)).astype(BF16)
        for h in range(heads):
            lanes = slice(h * HEAD, (h + 1) * HEAD)
            scores = jnp.where(causal, dot(near_q[:, lanes], near_k[:, lanes], ((1,), (1,))), 0.0)
            inside_out[span, lanes] = dot(scores.astype(BF16), value[:, lanes], ((1,), (0,)))
            state_out[n, h] = state[h]
            fade_out[n, h : h + 1] = jnp.exp(faded[h])
            added = dot(value[:, lanes], late_k[:, lanes], ((0,), (0,)))
            state[h] = jnp.exp(ending[:, lanes]) * state[h] + added
            faded[h] = faded[h] + ending[:, lanes]
    for h in range(heads):
        last_out[h] = state[h]
        total_out[h] = jnp.exp(faded[h])


def gate_kernel(*refs, where, rows):
    normed = refs[0]
    shards = refs[1 : 1 + len(where)]
    gate_out, pool_out, tail_out, whole = refs[1 + len(where) :]
    assemble(shards, where, whole, rows)
    width = gate_out.shape[1]
    projected = dot(normed[...], whole[...], ((1,), (0,))).astype(BF16)
    gate_out[...] = projected[:, :width]
    pool_out[...] = projected[:, width:]
    tail_out[...] = projected[projected.shape[0] - WIDEST :, width:]


def close_kernel(*refs, where, rows):
    inside, reach, states, fades, entering, gate, head_gain, pool_in, border, mapping, scale = refs[:11]
    shards = refs[11 : 11 + len(where)]
    keep_out, far_out, send_out, whole, joined, extended = refs[11 + len(where) :]
    assemble(shards, where, whole, rows)
    length, width = inside.shape
    heads = width // HEAD
    sp, tp = lax.axis_index("sp"), lax.axis_index("tp")
    part, pair = sp % PAIR, sp // PAIR
    for n in range(length // BLOCK):
        span = slice(n * BLOCK, (n + 1) * BLOCK)
        for h in range(heads):
            lanes = slice(h * HEAD, (h + 1) * HEAD)
            memory = states[n, h] + fades[n, h : h + 1] * entering[h]
            raw = inside[span, lanes] + dot(reach[span, lanes], memory.astype(BF16), ((1,), (1,)))
            level = lax.rsqrt(jnp.mean(raw * raw, axis=1, keepdims=True) + EPSILON)
            gating = jax.nn.silu(gate[span, lanes].astype(F32))
            joined[span, lanes] = (raw * level * head_gain[...] * gating).astype(BF16)
    extended[0:WIDEST, :] = border[...].astype(F32)
    extended[WIDEST:, :] = pool_in[...].astype(F32)
    sums = extended[...]
    grouping = tp * PAIR + part
    chosen = jnp.zeros((length, width), F32)
    step = 1
    for level in range(4):
        sums = sums[step:, :] + sums[:-step, :]
        step *= 2
        chosen = jnp.where(grouping == level, sums[sums.shape[0] - length :, :], chosen)
    reach_span = jnp.left_shift(jnp.int32(2), grouping)
    position = pair * length + lax.broadcasted_iota(jnp.int32, (length, 1), 0)
    amount = jnp.minimum(position + 1, reach_span).astype(F32)
    pooled = (chosen / amount - extended[WIDEST:, :]).astype(BF16)
    mapped = dot(pooled, mapping[...], ((1,), (0,)))
    joined[:, width:] = (mapped * scale[...]).astype(BF16)
    quarter = keep_out.shape[0]
    mixed = functools.partial(dot, contract=((1,), (1,)))

    def rows_of(owner_part, owner_tp):
        spot = (owner_part * 2 + owner_tp) * quarter
        return joined[pl.ds(pl.multiple_of(spot, quarter), quarter), :]

    send_out[0:quarter, :] = mixed(rows_of(part, 1 - tp), whole[...]).astype(BF16)
    send_out[quarter:, :] = mixed(rows_of(1 - part, 1 - tp), whole[...]).astype(BF16)
    far_out[...] = mixed(rows_of(1 - part, tp), whole[...]).astype(BF16)
    keep_out[...] = mixed(rows_of(part, tp), whole[...]).astype(BF16)


def per_device(
    tokens,
    norm_gain,
    query_weight,
    forget_weight,
    value_weight,
    outgate_weight,
    pool_in_weight,
    forget_room,
    decay_shift,
    head_gain,
    start_state,
    pool_map,
    pool_scale,
    out_rec_weight,
    out_pool_weight,
):
    n_sp, n_fs = lax.axis_size("sp"), lax.axis_size("fs")
    sp = lax.axis_index("sp")
    part, pair = sp % PAIR, sp // PAIR
    model = norm_gain.shape[0]
    columns = query_weight.shape[1] // PAIR
    heads = columns // HEAD
    length = tokens.shape[1] * PAIR

    def columns_of(weights, which):
        return jnp.concatenate(
            [lax.dynamic_slice_in_dim(w, which * columns, columns, axis=1) for w in weights], axis=1
        )

    def rows_of(weights, which):
        return jnp.concatenate(
            [lax.dynamic_slice_in_dim(w, which * columns, columns, axis=0) for w in weights], axis=0
        ).T

    def local(value, axis, size):
        return lax.dynamic_slice_in_dim(value, part * size, size, axis=axis)

    half = n_sp // 2
    fine = [g for g in ([0], [1], list(range(2, half)), list(range(half, n_sp))) if g]
    coarse = [list(range(n_sp))]

    def spread_of(take, weights, groups):
        pieces = spread(take(weights, part), take(weights, 1 - part), groups)
        return [piece[0] for piece in pieces], [piece[1:] for piece in pieces]

    mine = tokens[0]
    near = swapped(mine, "sp", 1)
    mix_shards, mix_where = spread_of(columns_of, (forget_weight, query_weight, value_weight), fine)
    gate_shards, gate_where = spread_of(columns_of, (outgate_weight, pool_in_weight), coarse)
    out_shards, out_where = spread_of(rows_of, (out_rec_weight, out_pool_weight), coarse)
    mine_other = swapped(mine, "tp", 1)
    near_other = swapped(near, "tp", 1)
    (normed,) = call(
        norm_kernel,
        [((length, model), BF16)],
        mine,
        near,
        mine_other,
        near_other,
        norm_gain[None],
        name="norm",
    )
    shift_near = swapped(decay_shift[0].astype(F32), "sp", 1)
    first = jnp.where(part == 0, decay_shift[0], shift_near)
    second = jnp.where(part == 0, shift_near, decay_shift[0])
    shift = local(jnp.concatenate([first, second], axis=0), 1, heads)
    blocks = length // BLOCK
    rows = query_weight.shape[0]
    inside, reach, states, fades, total, last = call(
        functools.partial(mix_kernel, where=mix_where, rows=rows),
        [
            ((length, columns), F32),
            ((length, columns), BF16),
            ((blocks, heads, HEAD, HEAD), F32),
            ((blocks, heads, HEAD), F32),
            ((heads, 1, HEAD), F32),
            ((heads, HEAD, HEAD), F32),
        ],
        normed,
        local(forget_room, 0, columns)[None],
        shift,
        *mix_shards,
        scratch=[pltpu.VMEM((model, 3 * columns), BF16)],
        name="mix",
    )
    opening = local(start_state[0], 0, heads).transpose(0, 2, 1)
    entering = opening

    def handoff(turn, entering):
        arrived = passed_on((total * entering + last).astype(BF16), "sp", PAIR).astype(F32)
        return jnp.where(pair == 0, opening, arrived)

    if n_sp // PAIR <= 4:
        for turn in range(n_sp // PAIR - 1):
            entering = handoff(turn, entering)
    else:
        entering = lax.fori_loop(0, n_sp // PAIR - 1, handoff, entering)
    gate, pool_in, tail = call(
        functools.partial(gate_kernel, where=gate_where, rows=rows),
        [((length, columns), BF16), ((length, columns), BF16), ((WIDEST, columns), BF16)],
        normed,
        *gate_shards,
        scratch=[pltpu.VMEM((model, 2 * columns), BF16)],
        name="gate",
    )
    border = passed_on(tail, "sp", PAIR)
    quarter = length // (PAIR * 2)
    keep, far, send = call(
        functools.partial(close_kernel, where=out_where, rows=out_rec_weight.shape[1]),
        [((quarter, model), BF16), ((quarter, model), BF16), ((2 * quarter, model), BF16)],
        inside,
        reach,
        states,
        fades,
        entering,
        gate,
        head_gain[None],
        pool_in,
        border,
        local(pool_map, 0, 1)[0],
        local(pool_scale, 0, columns)[None],
        *out_shards,
        scratch=[
            pltpu.VMEM((model, 2 * columns), BF16),
            pltpu.VMEM((length, 2 * columns), BF16),
            pltpu.VMEM((WIDEST + length, columns), F32),
        ],
        name="close",
    )
    met = swapped(send, "tp", 1).astype(F32)
    owed = (far.astype(F32) + met[quarter:]).astype(BF16)
    back = swapped(owed, "sp", 1).astype(F32)
    return (keep.astype(F32) + met[:quarter] + back).astype(BF16)[None]


def solution(mesh):
    return jax.shard_map(
        per_device,
        mesh=mesh,
        in_specs=(
            P("fs", "sp", "tp"),
            P(),
            P(("sp", "fs"), "tp"),
            P(("sp", "fs"), "tp"),
            P(("sp", "fs"), "tp"),
            P(("sp", "fs"), "tp"),
            P(("sp", "fs"), "tp"),
            P("tp"),
            P("fs", "sp", "tp"),
            P(),
            P("fs", "tp", None, None),
            P("tp", None, None),
            P("tp"),
            P("tp", ("sp", "fs")),
            P("tp", ("sp", "fs")),
        ),
        out_specs=P("fs", ("sp", "tp"), None),
        check_vma=False,
    )
```

```python
import functools

import jax
import jax.numpy as jnp
from jax import lax
from jax.experimental import pallas as pl
from jax.experimental.pallas import tpu as pltpu
from jax.sharding import PartitionSpec as P


HEAD = 128
WIDEST = 16
BLOCK = 128
PAIR = 2
EPSILON = 1e-06
F32 = jnp.float32
BF16 = jnp.bfloat16


def dot(a, b, contract):
    return lax.dot_general(a, b, (contract, ((), ())), preferred_element_type=F32)


def swapped(value, axis, distance):
    count = lax.axis_size(axis)
    return lax.ppermute(value, axis, [(i, i ^ distance) for i in range(count)])


def passed_on(value, axis, steps, first=0, stride=1):
    count = lax.axis_size(axis)
    return lax.ppermute(value, axis, [(i, i + steps) for i in range(first, count - steps, stride)])


def call(kernel, outs, *args, scratch=(), outside=(), room=24):
    vmem = pl.BlockSpec(memory_space=pltpu.VMEM)
    anywhere = pl.BlockSpec(memory_space=pltpu.HBM)
    return pl.pallas_call(
        kernel,
        out_shape=[jax.ShapeDtypeStruct(shape, dtype) for shape, dtype in outs],
        in_specs=[anywhere if k in outside else vmem for k in range(len(args))],
        out_specs=[vmem] * len(outs),
        scratch_shapes=list(scratch),
        compiler_params=pltpu.CompilerParams(vmem_limit_bytes=room * 2**20),
    )(*args)


def along_line(same, other):
    return [same] + [swapped(other if d % PAIR else same, "sp", d) for d in range(1, lax.axis_size("sp"))]


def over_plane(arrived, groups, routes):
    pieces = []
    for group, route in zip(groups, routes):
        plane = arrived[group[0]] if len(group) == 1 else jnp.concatenate([arrived[d] for d in group], axis=0)
        by_x = swapped(plane, "fs", 1)
        by_y = swapped(plane, "fs", 2)
        if route == "x":
            across = swapped(by_y, "fs", 1)
        else:
            across = swapped(by_x, "fs", 2)
        for c, piece in enumerate((plane, by_x, by_y, across)):
            pieces.append((piece, c, tuple(group)))
    return pieces


def split(pieces):
    return [piece[0] for piece in pieces], tuple(piece[1:] for piece in pieces)


def assemble(refs, where, whole, rows, leading=0):
    sp, fs, n_fs = lax.axis_index("sp"), lax.axis_index("fs"), lax.axis_size("fs")
    for ref, (c, distances) in zip(refs, where):
        for k, d in enumerate(distances):
            block = (d // PAIR - leading) * PAIR * n_fs * rows
            spot = block + (((sp ^ d) % PAIR) * n_fs + (fs ^ c)) * rows
            whole[pl.ds(pl.multiple_of(spot, rows), rows), :] = ref[k * rows : (k + 1) * rows, :]


def projected_by(normed, whole, rows, leading):
    pair, wide = lax.axis_index("sp") // PAIR, PAIR * lax.axis_size("fs") * rows
    total = None
    for k in range(whole.shape[0] // wide):
        features = pl.ds(pl.multiple_of((pair ^ (k + leading)) * wide, wide), wide)
        part = dot(normed[:, features], whole[k * wide : (k + 1) * wide, :], ((1,), (0,)))
        total = part if total is None else total + part
    return total


def pack_kernel(*refs):
    sources, (same, other), sems = refs[:-3], refs[-3:-1], refs[-1]
    part = lax.axis_index("sp") % PAIR
    columns = sources[0].shape[1] // PAIR
    copies = []
    for j, (target, which) in enumerate(((same, part), (other, 1 - part))):
        for k, source in enumerate(sources):
            cut = source.at[:, pl.ds(pl.multiple_of(which * columns, columns), columns)]
            place = target.at[:, k * columns : (k + 1) * columns]
            copies.append(pltpu.make_async_copy(cut, place, sems.at[j, k]))
    for copy in copies:
        copy.start()
    for copy in copies:
        copy.wait()


def pack_rows_kernel(*refs):
    sources, (same, other), held, sems = refs[:-4], refs[-4:-2], refs[-2], refs[-1]
    part = lax.axis_index("sp") % PAIR
    rows = sources[0].shape[0] // PAIR
    copies = []
    for k, source in enumerate(sources):
        copies.append(pltpu.make_async_copy(source, held.at[k], sems.at[k]))
    for copy in copies:
        copy.start()
    for copy in copies:
        copy.wait()
    for target, which in ((same, part), (other, 1 - part)):
        for k in range(len(sources)):
            cut = held[k, pl.ds(pl.multiple_of(which * rows, rows), rows), :]
            target[:, k * rows : (k + 1) * rows] = cut.T


def norm_kernel(mine, mine_other, gain, own_out, other_out, tail_out):
    tp = lax.axis_index("tp")
    width = mine.shape[1]
    here = pl.ds(pl.multiple_of(tp * width, width), width)
    there = pl.ds(pl.multiple_of((1 - tp) * width, width), width)
    a, b = mine[...].astype(F32), mine_other[...].astype(F32)
    total = jnp.sum(a * a, axis=1, keepdims=True) + jnp.sum(b * b, axis=1, keepdims=True)
    scale = lax.rsqrt(total / (2 * width) + EPSILON)
    own = (a * scale * gain[:, here]).astype(BF16)
    own_out[...] = own
    tail_out[...] = own[own.shape[0] - WIDEST :, :]
    other_out[...] = (b * scale * gain[:, there]).astype(BF16)


def merge_kernel(adjacent, second, out):
    out[...] = adjacent[...] + second[...]


def cumulative(ones_below, value):
    high = value.astype(BF16)
    rest = value - high.astype(F32)
    middle = rest.astype(BF16)
    low = (rest - middle.astype(F32)).astype(BF16)
    contract = ((1,), (0,))
    return dot(ones_below, high, contract) + (dot(ones_below, middle, contract) + dot(ones_below, low, contract))


def first_kernel(*refs, where, rows):
    mine, mine_other, near, near_other, before, before_other = refs[:6]
    shards, (normed, sum_out, whole) = refs[6:-3], refs[-3:]
    part, tp = lax.axis_index("sp") % PAIR, lax.axis_index("tp")
    length, width = mine.shape
    here = pl.ds(pl.multiple_of(tp * width, width), width)
    there = pl.ds(pl.multiple_of((1 - tp) * width, width), width)
    for spot, left, right in ((part, mine, mine_other), (1 - part, near, near_other)):
        place = pl.ds(pl.multiple_of(spot * length, length), length)
        normed[place, here] = left[...]
        normed[place, there] = right[...]
    normed[PAIR * length :, here] = before[...]
    normed[PAIR * length :, there] = before_other[...]
    assemble(shards, where, whole, rows)
    sum_out[...] = projected_by(normed, whole, rows, 0)


def mix_kernel(*refs, where, rows):
    normed, earlier, room_whole, shift_mine, shift_near, start = refs[:6]
    shards = refs[6 : 6 + len(where)]
    projected_out, keyed_out, within_out, state_out, fade_out, leaving_out, opening_out, total_out, last_out, border_out = refs[
        6 + len(where) : 16 + len(where)
    ]
    whole, shift, first, sem = refs[16 + len(where) :]
    part = lax.axis_index("sp") % PAIR
    length, width = keyed_out.shape
    heads = width // HEAD
    fetch = pltpu.make_async_copy(start.at[pl.ds(part * heads, heads)], first, sem)
    fetch.start()
    lines, own = shift_mine.shape
    shift[...] = jnp.zeros_like(shift)
    shift[0:lines, pl.ds(pl.multiple_of(part * own, own), own)] = shift_mine[...]
    shift[0:lines, pl.ds(pl.multiple_of((1 - part) * own, own), own)] = shift_near[...]
    shifts = shift[...].T
    assemble(shards, where, whole, rows, 1)
    projected = (earlier[...] + projected_by(normed, whole, rows, 1)).astype(BF16)
    projected_out[...] = projected[0:length, :]
    border_out[...] = projected[length:, 4 * width :]
    room = room_whole[:, pl.ds(pl.multiple_of(part * width, width), width)]
    t = lax.broadcasted_iota(jnp.int32, (BLOCK, BLOCK), 0)
    s = lax.broadcasted_iota(jnp.int32, (BLOCK, BLOCK), 1)
    ones_below = (s <= t).astype(F32).astype(BF16)
    state = [jnp.zeros((HEAD, HEAD), F32) for _ in range(heads)]
    faded = [jnp.zeros((1, HEAD), F32) for _ in range(heads)]
    for n in range(length // BLOCK):
        span = slice(n * BLOCK, (n + 1) * BLOCK)
        logits = projected[span, 0:width].astype(F32)
        value = projected[span, 2 * width : 3 * width]
        keyed = room * (1.0 - jax.nn.sigmoid(logits))
        every = shifts[span, :]
        lags = [
            jnp.where(part == 0, every[:, h : h + 1], every[:, heads + h : heads + h + 1]) for h in range(heads)
        ]
        lag = jnp.concatenate([jnp.broadcast_to(column, (BLOCK, HEAD)) for column in lags], axis=1)
        within = cumulative(ones_below, jnp.log1p(-keyed) + lag)
        keyed_out[span, :] = keyed
        within_out[span, :] = within
        ending = within[BLOCK - 1 : BLOCK]
        late_k = (keyed * jnp.exp(ending - within)).astype(BF16)
        for h in range(heads):
            lanes = slice(h * HEAD, (h + 1) * HEAD)
            state_out[n, h] = state[h]
            fade_out[n, h : h + 1] = jnp.exp(faded[h])
            added = dot(value[:, lanes], late_k[:, lanes], ((0,), (0,)))
            state[h] = jnp.exp(ending[:, lanes]) * state[h] + added
            faded[h] = faded[h] + ending[:, lanes]
    fetch.wait()
    for h in range(heads):
        total = jnp.exp(faded[h])
        opening = first[h].T
        opening_out[h] = opening
        leaving_out[h] = (total * opening + state[h]).astype(BF16)
        last_out[h] = state[h]
        total_out[h] = total


def inside_kernel(projected, keyed, within_all, inside_out, reach_out):
    length, width = keyed.shape
    t = lax.broadcasted_iota(jnp.int32, (BLOCK, BLOCK), 0)
    s = lax.broadcasted_iota(jnp.int32, (BLOCK, BLOCK), 1)
    causal = s <= t
    for n in range(length // BLOCK):
        span = slice(n * BLOCK, (n + 1) * BLOCK)
        queries = jax.nn.silu(projected[span, width : 2 * width].astype(F32)) * HEAD ** (-0.5)
        value = projected[span, 2 * width : 3 * width]
        within = within_all[span, :]
        centre = within[BLOCK // 2 - 1 : BLOCK // 2]
        near_q = (queries * jnp.exp(within - centre)).astype(BF16)
        near_k = (keyed[span, :] * jnp.exp(centre - within)).astype(BF16)
        reach_out[span, :] = (queries * jnp.exp(within)).astype(BF16)
        for h in range(width // HEAD):
            lanes = slice(h * HEAD, (h + 1) * HEAD)
            scores = jnp.where(causal, dot(near_q[:, lanes], near_k[:, lanes], ((1,), (1,))), 0.0)
            inside_out[span, lanes] = dot(scores.astype(BF16), value[:, lanes], ((1,), (0,)))


def join_kernel(
    inside, reach, states, fades, opening, arrived, projected, head_gain, border, mappings, scales, joined, extended
):
    length, width = inside.shape
    heads = width // HEAD
    sp, tp = lax.axis_index("sp"), lax.axis_index("tp")
    part, pair = sp % PAIR, sp // PAIR
    for h in range(heads):
        lanes = slice(h * HEAD, (h + 1) * HEAD)
        entering = jnp.where(pair == 0, opening[h], arrived[h].astype(F32))
        for n in range(length // BLOCK):
            span = slice(n * BLOCK, (n + 1) * BLOCK)
            memory = states[n, h] + fades[n, h : h + 1] * entering
            raw = inside[span, lanes] + dot(reach[span, lanes], memory.astype(BF16), ((1,), (1,)))
            level = lax.rsqrt(jnp.mean(raw * raw, axis=1, keepdims=True) + EPSILON)
            gating = jax.nn.silu(projected[span, 3 * width + h * HEAD : 3 * width + (h + 1) * HEAD].astype(F32))
            joined[span, lanes] = (raw * level * head_gain[...] * gating).astype(BF16)
    extended[0:WIDEST, :] = border[...].astype(F32)
    extended[WIDEST:, :] = projected[:, 4 * width :].astype(F32)
    sums = extended[...]
    grouping = tp * PAIR + part
    chosen = jnp.zeros((length, width), F32)
    step = 1
    for level in range(4):
        sums = sums[step:, :] + sums[:-step, :]
        step *= 2
        chosen = jnp.where(grouping == level, sums[sums.shape[0] - length :, :], chosen)
    span_length = jnp.left_shift(jnp.int32(2), grouping)
    position = pair * length + lax.broadcasted_iota(jnp.int32, (length, 1), 0)
    amount = jnp.minimum(position + 1, span_length).astype(F32)
    pooled = (chosen / amount - extended[WIDEST:, :]).astype(BF16)
    mapped = dot(pooled, mappings[part], ((1,), (0,)))
    scale = scales[:, pl.ds(pl.multiple_of(part * width, width), width)]
    joined[:, width:] = (mapped * scale).astype(BF16)


def out_kernel(*refs, count, sort):
    joined = refs[0]
    shards = refs[1 : 1 + count]
    keep_out, far_out, send_out, whole = refs[1 + count :]
    part, tp = lax.axis_index("sp") % PAIR, lax.axis_index("tp")
    quarter = keep_out.shape[0]
    if sort is None:
        spot = 0
        for shard in shards:
            whole[spot : spot + shard.shape[0], :] = shard[...]
            spot += shard.shape[0]
    else:
        where, rows = sort
        sp, fs, n_fs = lax.axis_index("sp"), lax.axis_index("fs"), lax.axis_size("fs")
        for shard, (c, distances) in zip(shards, where):
            for k, d in enumerate(distances):
                spot = ((sp ^ d) * n_fs + (fs ^ c)) * rows
                whole[pl.ds(pl.multiple_of(spot, rows), rows), :] = shard[k * rows : (k + 1) * rows, :]

    def mixed(owner_part, owner_tp):
        spot = (owner_part * 2 + owner_tp) * quarter
        return dot(joined[pl.ds(pl.multiple_of(spot, quarter), quarter), :], whole[...], ((1,), (1,)))

    send_out[0:quarter, :] = mixed(part, 1 - tp).astype(BF16)
    send_out[quarter:, :] = mixed(1 - part, 1 - tp).astype(BF16)
    far_out[...] = mixed(1 - part, tp).astype(BF16)
    keep_out[...] = mixed(part, tp).astype(BF16)


def final_kernel(*refs, order, columns):
    out = refs[-1]
    sp, fs, n_fs = lax.axis_index("sp"), lax.axis_index("fs"), lax.axis_size("fs")
    quarter = out.shape[0]
    for k, places in enumerate(order):
        keep, met, back = refs[3 * k : 3 * k + 3]
        if places is None:
            out[...] = (keep[...].astype(F32) + met[0:quarter].astype(F32) + back[...].astype(F32)).astype(BF16)
            continue
        for j, (c, d) in enumerate(places):
            twin = places.index((c, d ^ 1))
            lanes = slice(j * columns, (j + 1) * columns)
            other = slice(twin * columns, (twin + 1) * columns)
            value = keep[:, lanes].astype(F32) + met[0:quarter, lanes].astype(F32) + back[:, other].astype(F32)
            spot = ((sp ^ d) * n_fs + (fs ^ c)) * columns
            out[:, pl.ds(pl.multiple_of(spot, columns), columns)] = value.astype(BF16)


def per_device(
    tokens,
    norm_gain,
    query_weight,
    forget_weight,
    value_weight,
    outgate_weight,
    pool_in_weight,
    forget_room,
    decay_shift,
    head_gain,
    start_state,
    pool_map,
    pool_scale,
    out_rec_weight,
    out_pool_weight,
):
    n_sp, n_fs = lax.axis_size("sp"), lax.axis_size("fs")
    pair = lax.axis_index("sp") // PAIR
    model = norm_gain.shape[0]
    rows = query_weight.shape[0]
    columns = query_weight.shape[1] // PAIR
    heads = columns // HEAD
    length = tokens.shape[1] * PAIR
    blocks = length // BLOCK
    mine = tokens[0]
    mine_other = swapped(mine, "tp", 1)
    pack_out = [((rows, 5 * columns), BF16)] * 2
    mix_same, mix_other = call(
        pack_kernel,
        pack_out,
        forget_weight,
        query_weight,
        value_weight,
        outgate_weight,
        pool_in_weight,
        scratch=[pltpu.SemaphoreType.DMA((2, 5))],
        outside=range(5),
        room=62,
    )
    line_a = along_line(mix_same, mix_other)
    pack_out = [((out_rec_weight.shape[1], 2 * columns), BF16)] * 2
    out_same, out_other = call(
        pack_rows_kernel,
        pack_out,
        out_rec_weight,
        out_pool_weight,
        scratch=[pltpu.VMEM((2,) + out_rec_weight.shape, BF16), pltpu.SemaphoreType.DMA((2,))],
        outside=range(2),
        room=62,
    )
    half = ((tokens.shape[1], tokens.shape[2]), BF16)
    tail = ((WIDEST, tokens.shape[2]), BF16)
    normed_own, normed_other, ends = call(norm_kernel, [half, half, tail], mine, mine_other, norm_gain[None])
    (before,) = call(merge_kernel, [tail], passed_on(ends, "sp", 1, 1, PAIR), passed_on(ends, "sp", 2, 1, PAIR))
    before_other = swapped(before, "tp", 1)
    near = swapped(normed_own, "sp", 1)
    shift_mine = decay_shift[0].T
    shift_near = swapped(shift_mine, "sp", 1)
    line_c = along_line(out_same, out_other)
    cut = (n_sp + 2) // 2
    fine = [[0], [1], list(range(2, cut)), list(range(cut, n_sp))]
    coarse = [[0], [1], list(range(2, n_sp))]
    mix_pieces = over_plane(line_a, fine, "xyyx")
    first_shards, first_where = split([p for p in mix_pieces if p[2][0] < PAIR])
    mix_shards, mix_where = split([p for p in mix_pieces if p[2][0] >= PAIR])
    out_pieces = over_plane(line_c, coarse, "yyx")
    near_other = swapped(near, "tp", 1)
    wide = PAIR * n_fs * rows
    normed, earlier = call(
        functools.partial(first_kernel, where=first_where, rows=rows),
        [((length + WIDEST, model), BF16), ((length + WIDEST, 5 * columns), F32)],
        normed_own,
        normed_other,
        near,
        near_other,
        before,
        before_other,
        *first_shards,
        scratch=[pltpu.VMEM((wide, 5 * columns), BF16)],
    )
    projected, keyed, within, states, fades, leaving, opening, total, last, border = call(
        functools.partial(mix_kernel, where=mix_where, rows=rows),
        [
            ((length, 5 * columns), BF16),
            ((length, columns), F32),
            ((length, columns), F32),
            ((blocks, heads, HEAD, HEAD), F32),
            ((blocks, heads, HEAD), F32),
            ((heads, HEAD, HEAD), BF16),
            ((heads, HEAD, HEAD), F32),
            ((heads, 1, HEAD), F32),
            ((heads, HEAD, HEAD), F32),
            ((WIDEST, columns), BF16),
        ],
        normed,
        earlier,
        forget_room[None],
        shift_mine,
        shift_near,
        start_state[0],
        *mix_shards,
        scratch=[
            pltpu.VMEM((model - wide, 5 * columns), BF16),
            pltpu.VMEM((8, length), F32),
            pltpu.VMEM((heads, HEAD, HEAD), F32),
            pltpu.SemaphoreType.DMA(()),
        ],
        outside=(5,),
        room=30,
    )
    arrived = passed_on(leaving, "sp", PAIR)

    def handoff(turn, arrived):
        onward = (total * arrived.astype(F32) + last).astype(BF16)
        onward = jnp.where(pair == 0, leaving, onward)
        return passed_on(onward, "sp", PAIR)

    if n_sp // PAIR > 2:
        arrived = lax.fori_loop(0, n_sp // PAIR - 2, handoff, arrived)
    inside, reach = call(inside_kernel, [((length, columns), F32), ((length, columns), BF16)], projected, keyed, within)
    (joined,) = call(
        join_kernel,
        [((length, 2 * columns), BF16)],
        inside,
        reach,
        states,
        fades,
        opening,
        arrived,
        projected,
        head_gain[None],
        border,
        pool_map,
        pool_scale[None],
        scratch=[pltpu.VMEM((WIDEST + length, columns), F32)],
    )
    quarter = length // (PAIR * 2)
    out_rows = out_rec_weight.shape[1]
    if out_rows % 128:
        sets = [out_pieces]
    else:
        sets = [[p for p in out_pieces if p[1] in near_by] for near_by in ((0, 1, 2), (3,))]
    shares, order = [], []
    for pieces in sets:
        shards, where = split(pieces)
        sort = (where, out_rows) if out_rows % 128 else None
        wide = sum(shard.shape[0] for shard in shards)
        keep, far, send = call(
            functools.partial(out_kernel, count=len(shards), sort=sort),
            [((quarter, wide), BF16), ((quarter, wide), BF16), ((2 * quarter, wide), BF16)],
            joined,
            *shards,
            scratch=[pltpu.VMEM((wide, 2 * columns), BF16)],
        )
        met = swapped(send, "tp", 1)
        owed = (far.astype(F32) + met[quarter:].astype(F32)).astype(BF16)
        shares += [keep, met, swapped(owed, "sp", 1)]
        order.append(None if sort else tuple((c, d) for c, group in where for d in group))
    (mixed,) = call(
        functools.partial(final_kernel, order=tuple(order), columns=out_rows), [((quarter, model), BF16)], *shares
    )
    return mixed[None]


def solution(mesh):
    return jax.shard_map(
        per_device,
        mesh=mesh,
        in_specs=(
            P("fs", "sp", "tp"),
            P(),
            P(("sp", "fs"), "tp"),
            P(("sp", "fs"), "tp"),
            P(("sp", "fs"), "tp"),
            P(("sp", "fs"), "tp"),
            P(("sp", "fs"), "tp"),
            P("tp"),
            P("fs", "sp", "tp"),
            P(),
            P("fs", "tp", None, None),
            P("tp", None, None),
            P("tp"),
            P("tp", ("sp", "fs")),
            P("tp", ("sp", "fs")),
        ),
        out_specs=P("fs", ("sp", "tp"), None),
        check_vma=False,
    )
```

```python
import functools

import jax
import jax.numpy as jnp
from jax import lax
from jax.experimental import pallas as pl
from jax.experimental.pallas import tpu as pltpu
from jax.sharding import PartitionSpec as P


HEAD = 128
WIDEST = 16
BLOCK = 128
PAIR = 2
EPSILON = 1e-06
F32 = jnp.float32
BF16 = jnp.bfloat16


def dot(a, b, contract):
    return lax.dot_general(a, b, (contract, ((), ())), preferred_element_type=F32)


def swapped(value, axis, distance):
    count = lax.axis_size(axis)
    return lax.ppermute(value, axis, [(i, i ^ distance) for i in range(count)])


def passed_on(value, axis, steps, first=0, stride=1):
    count = lax.axis_size(axis)
    return lax.ppermute(value, axis, [(i, i + steps) for i in range(first, count - steps, stride)])


def call(kernel, outs, *args, scratch=(), outside=(), room=16):
    vmem = pl.BlockSpec(memory_space=pltpu.VMEM)
    anywhere = pl.BlockSpec(memory_space=pltpu.HBM)
    return pl.pallas_call(
        kernel,
        out_shape=[jax.ShapeDtypeStruct(shape, dtype) for shape, dtype in outs],
        in_specs=[anywhere if k in outside else vmem for k in range(len(args))],
        out_specs=[vmem] * len(outs),
        scratch_shapes=list(scratch),
        compiler_params=pltpu.CompilerParams(vmem_limit_bytes=room * 2**20),
    )(*args)


def along_line(same, other):
    return [same] + [swapped(other if d % PAIR else same, "sp", d) for d in range(1, lax.axis_size("sp"))]


def over_plane(arrived, groups, routes):
    pieces = []
    for group, route in zip(groups, routes):
        plane = arrived[group[0]]
        if len(group) > 1:
            shape = (len(group) * plane.shape[0], plane.shape[1])
            (plane,) = call(stack_kernel, [(shape, BF16)], *(arrived[d] for d in group))
        by_x = swapped(plane, "fs", 1)
        by_y = swapped(plane, "fs", 2)
        if route == "x":
            across = swapped(by_y, "fs", 1)
        else:
            across = swapped(by_x, "fs", 2)
        for c, piece in enumerate((plane, by_x, by_y, across)):
            pieces.append((piece, c, tuple(group)))
    return pieces


def stack_kernel(*refs):
    pieces, out = refs[:-1], refs[-1]
    rows = pieces[0].shape[0]
    for k, piece in enumerate(pieces):
        out[k * rows : (k + 1) * rows, :] = piece[...]


def split(pieces):
    return [piece[0] for piece in pieces], tuple(piece[1:] for piece in pieces)


def assemble(refs, where, whole, rows, leading=0, first=0):
    sp, fs, n_fs = lax.axis_index("sp"), lax.axis_index("fs"), lax.axis_size("fs")
    for ref, (c, distances) in zip(refs, where):
        for k, d in enumerate(distances):
            block = (d // PAIR - leading) * PAIR * n_fs * rows
            spot = block + (((sp ^ d) % PAIR) * n_fs + (fs ^ c)) * rows
            cut = ref[k * rows : (k + 1) * rows, first : first + whole.shape[1]]
            whole[pl.ds(pl.multiple_of(spot, rows), rows), :] = cut


def projected_by(normed, whole, rows, leading, upto=None):
    pair, wide = lax.axis_index("sp") // PAIR, PAIR * lax.axis_size("fs") * rows
    total = None
    for k in range(whole.shape[0] // wide):
        features = pl.ds(pl.multiple_of((pair ^ (k + leading)) * wide, wide), wide)
        part = dot(normed[0 : upto or normed.shape[0], features], whole[k * wide : (k + 1) * wide, :], ((1,), (0,)))
        total = part if total is None else total + part
    return total


def pack_kernel(*refs):
    sources, (same, other), sems = refs[:-3], refs[-3:-1], refs[-1]
    part = lax.axis_index("sp") % PAIR
    columns = sources[0].shape[1] // PAIR
    copies = []
    for j, (target, which) in enumerate(((same, part), (other, 1 - part))):
        for k, source in enumerate(sources):
            cut = source.at[:, pl.ds(pl.multiple_of(which * columns, columns), columns)]
            place = target.at[:, k * columns : (k + 1) * columns]
            copies.append(pltpu.make_async_copy(cut, place, sems.at[j, k]))
    for copy in copies:
        copy.start()
    for copy in copies:
        copy.wait()


def pack_rows_kernel(*refs):
    sources, (same, other), held, sems = refs[:-4], refs[-4:-2], refs[-2], refs[-1]
    part = lax.axis_index("sp") % PAIR
    rows = sources[0].shape[0] // PAIR
    copies = []
    for k, source in enumerate(sources):
        copies.append(pltpu.make_async_copy(source, held.at[k], sems.at[k]))
    for copy in copies:
        copy.start()
    for copy in copies:
        copy.wait()
    for target, which in ((same, part), (other, 1 - part)):
        for k in range(len(sources)):
            cut = held[k, pl.ds(pl.multiple_of(which * rows, rows), rows), :]
            target[:, k * rows : (k + 1) * rows] = cut.T


def norm_kernel(mine, mine_other, gain, own_out, other_out, tail_out):
    tp = lax.axis_index("tp")
    width = mine.shape[1]
    here = pl.ds(pl.multiple_of(tp * width, width), width)
    there = pl.ds(pl.multiple_of((1 - tp) * width, width), width)
    a, b = mine[...].astype(F32), mine_other[...].astype(F32)
    total = jnp.sum(a * a, axis=1, keepdims=True) + jnp.sum(b * b, axis=1, keepdims=True)
    scale = lax.rsqrt(total / (2 * width) + EPSILON)
    own = (a * scale * gain[:, here]).astype(BF16)
    own_out[...] = own
    tail_out[...] = own[own.shape[0] - WIDEST :, :]
    other_out[...] = (b * scale * gain[:, there]).astype(BF16)


def merge_kernel(adjacent, second, out):
    out[...] = adjacent[...] + second[...]


def cumulative(ones_below, value):
    high = value.astype(BF16)
    rest = value - high.astype(F32)
    middle = rest.astype(BF16)
    low = (rest - middle.astype(F32)).astype(BF16)
    contract = ((1,), (0,))
    return dot(ones_below, high, contract) + (dot(ones_below, middle, contract) + dot(ones_below, low, contract))


def first_kernel(*refs, where, rows):
    mine, mine_other, near, near_other, before, before_other = refs[:6]
    shards, (normed, sum_out, whole) = refs[6:-3], refs[-3:]
    part, tp = lax.axis_index("sp") % PAIR, lax.axis_index("tp")
    length, width = mine.shape
    here = pl.ds(pl.multiple_of(tp * width, width), width)
    there = pl.ds(pl.multiple_of((1 - tp) * width, width), width)
    for spot, left, right in ((part, mine, mine_other), (1 - part, near, near_other)):
        place = pl.ds(pl.multiple_of(spot * length, length), length)
        normed[place, here] = left[...]
        normed[place, there] = right[...]
    normed[PAIR * length :, here] = before[...]
    normed[PAIR * length :, there] = before_other[...]
    assemble(shards, where, whole, rows)
    sum_out[...] = projected_by(normed, whole, rows, 0)


def mix_kernel(*refs, where, rows):
    normed, earlier, room_whole, shift_mine, shift_near, start = refs[:6]
    shards = refs[6 : 6 + len(where)]
    value_out, keyed_out, within_out, state_out, fade_out, leaving_out, opening_out, total_out, last_out = refs[
        6 + len(where) : 15 + len(where)
    ]
    whole, shift, first, sem = refs[15 + len(where) :]
    part = lax.axis_index("sp") % PAIR
    length, width = keyed_out.shape
    heads = width // HEAD
    fetch = pltpu.make_async_copy(start.at[pl.ds(part * heads, heads)], first, sem)
    fetch.start()
    lines, own = shift_mine.shape
    shift[...] = jnp.zeros_like(shift)
    shift[0:lines, pl.ds(pl.multiple_of(part * own, own), own)] = shift_mine[...]
    shift[0:lines, pl.ds(pl.multiple_of((1 - part) * own, own), own)] = shift_near[...]
    shifts = shift[...].T
    assemble(shards, where, whole, rows, 1)
    projected = earlier[0:length, 0 : 2 * width] + projected_by(normed, whole, rows, 1, length)
    projected = projected.astype(BF16)
    value_out[...] = projected[:, width:]
    room = room_whole[:, pl.ds(pl.multiple_of(part * width, width), width)]
    t = lax.broadcasted_iota(jnp.int32, (BLOCK, BLOCK), 0)
    s = lax.broadcasted_iota(jnp.int32, (BLOCK, BLOCK), 1)
    ones_below = (s <= t).astype(F32).astype(BF16)
    state = [jnp.zeros((HEAD, HEAD), F32) for _ in range(heads)]
    faded = [jnp.zeros((1, HEAD), F32) for _ in range(heads)]
    for n in range(length // BLOCK):
        span = slice(n * BLOCK, (n + 1) * BLOCK)
        logits = projected[span, 0:width].astype(F32)
        value = projected[span, width:]
        keyed = room * (1.0 - jax.nn.sigmoid(logits))
        every = shifts[span, :]
        lags = [
            jnp.where(part == 0, every[:, h : h + 1], every[:, heads + h : heads + h + 1]) for h in range(heads)
        ]
        lag = jnp.concatenate([jnp.broadcast_to(column, (BLOCK, HEAD)) for column in lags], axis=1)
        within = cumulative(ones_below, jnp.log1p(-keyed) + lag)
        keyed_out[span, :] = keyed
        within_out[span, :] = within
        ending = within[BLOCK - 1 : BLOCK]
        late_k = (keyed * jnp.exp(ending - within)).astype(BF16)
        for h in range(heads):
            lanes = slice(h * HEAD, (h + 1) * HEAD)
            state_out[n, h] = state[h]
            fade_out[n, h : h + 1] = jnp.exp(faded[h])
            added = dot(value[:, lanes], late_k[:, lanes], ((0,), (0,)))
            state[h] = jnp.exp(ending[:, lanes]) * state[h] + added
            faded[h] = faded[h] + ending[:, lanes]
    fetch.wait()
    for h in range(heads):
        total = jnp.exp(faded[h])
        opening = first[h].T
        opening_out[h] = opening
        leaving_out[h] = (total * opening + state[h]).astype(BF16)
        last_out[h] = state[h]
        total_out[h] = total


def inside_kernel(*refs, where, rows):
    normed, earlier, value_all, keyed, within_all = refs[:5]
    shards = refs[5 : 5 + len(where)]
    inside_out, reach_out, gate_out, pool_out, border_out, whole = refs[5 + len(where) :]
    length, width = keyed.shape
    assemble(shards, where, whole, rows, 1, 2 * width)
    projected = (earlier[:, 2 * width :] + projected_by(normed, whole, rows, 1)).astype(BF16)
    gate_out[...] = projected[0:length, width : 2 * width]
    pool_out[...] = projected[0:length, 2 * width :]
    border_out[...] = projected[length:, 2 * width :]
    t = lax.broadcasted_iota(jnp.int32, (BLOCK, BLOCK), 0)
    s = lax.broadcasted_iota(jnp.int32, (BLOCK, BLOCK), 1)
    causal = s <= t
    for n in range(length // BLOCK):
        span = slice(n * BLOCK, (n + 1) * BLOCK)
        queries = jax.nn.silu(projected[span, 0:width].astype(F32)) * HEAD ** (-0.5)
        value = value_all[span, :]
        within = within_all[span, :]
        centre = within[BLOCK // 2 - 1 : BLOCK // 2]
        near_q = (queries * jnp.exp(within - centre)).astype(BF16)
        near_k = (keyed[span, :] * jnp.exp(centre - within)).astype(BF16)
        reach_out[span, :] = (queries * jnp.exp(within)).astype(BF16)
        for h in range(width // HEAD):
            lanes = slice(h * HEAD, (h + 1) * HEAD)
            scores = jnp.where(causal, dot(near_q[:, lanes], near_k[:, lanes], ((1,), (1,))), 0.0)
            inside_out[span, lanes] = dot(scores.astype(BF16), value[:, lanes], ((1,), (0,)))


def join_kernel(
    inside, reach, states, fades, opening, arrived, gate, pool, head_gain, border, mappings, scales, joined, extended
):
    length, width = inside.shape
    heads = width // HEAD
    sp, tp = lax.axis_index("sp"), lax.axis_index("tp")
    part, pair = sp % PAIR, sp // PAIR
    for h in range(heads):
        lanes = slice(h * HEAD, (h + 1) * HEAD)
        entering = jnp.where(pair == 0, opening[h], arrived[h].astype(F32))
        for n in range(length // BLOCK):
            span = slice(n * BLOCK, (n + 1) * BLOCK)
            memory = states[n, h] + fades[n, h : h + 1] * entering
            raw = inside[span, lanes] + dot(reach[span, lanes], memory.astype(BF16), ((1,), (1,)))
            level = lax.rsqrt(jnp.mean(raw * raw, axis=1, keepdims=True) + EPSILON)
            gating = jax.nn.silu(gate[span, lanes].astype(F32))
            joined[span, lanes] = (raw * level * head_gain[...] * gating).astype(BF16)
    extended[0:WIDEST, :] = border[...].astype(F32)
    extended[WIDEST:, :] = pool[...].astype(F32)
    sums = extended[...]
    grouping = tp * PAIR + part
    chosen = jnp.zeros((length, width), F32)
    step = 1
    for level in range(4):
        sums = sums[step:, :] + sums[:-step, :]
        step *= 2
        chosen = jnp.where(grouping == level, sums[sums.shape[0] - length :, :], chosen)
    span_length = jnp.left_shift(jnp.int32(2), grouping)
    position = pair * length + lax.broadcasted_iota(jnp.int32, (length, 1), 0)
    amount = jnp.minimum(position + 1, span_length).astype(F32)
    pooled = (chosen / amount - extended[WIDEST:, :]).astype(BF16)
    mapped = dot(pooled, mappings[part], ((1,), (0,)))
    scale = scales[:, pl.ds(pl.multiple_of(part * width, width), width)]
    joined[:, width:] = (mapped * scale).astype(BF16)


def rows_owed(joined, whole, owner_part, owner_tp):
    quarter = joined.shape[0] // (PAIR * 2)
    rows = pl.ds(pl.multiple_of((owner_part * 2 + owner_tp) * quarter, quarter), quarter)
    return dot(joined[rows, :], whole[...], ((1,), (1,))).astype(BF16)


def send_kernel(*refs, count, sort):
    joined, shards = refs[0], refs[1 : 1 + count]
    send_out, whole = refs[1 + count :]
    part, tp = lax.axis_index("sp") % PAIR, lax.axis_index("tp")
    if sort is None:
        spot = 0
        for shard in shards:
            whole[spot : spot + shard.shape[0], :] = shard[...]
            spot += shard.shape[0]
    else:
        where, rows = sort
        sp, fs, n_fs = lax.axis_index("sp"), lax.axis_index("fs"), lax.axis_size("fs")
        for shard, (c, distances) in zip(shards, where):
            for k, d in enumerate(distances):
                spot = ((sp ^ d) * n_fs + (fs ^ c)) * rows
                whole[pl.ds(pl.multiple_of(spot, rows), rows), :] = shard[k * rows : (k + 1) * rows, :]
    quarter = send_out.shape[0] // 2
    send_out[0:quarter, :] = rows_owed(joined, whole, part, 1 - tp)
    send_out[quarter:, :] = rows_owed(joined, whole, 1 - part, 1 - tp)


def keep_kernel(joined, whole, keep_out, far_out):
    part, tp = lax.axis_index("sp") % PAIR, lax.axis_index("tp")
    far_out[...] = rows_owed(joined, whole, 1 - part, tp)
    keep_out[...] = rows_owed(joined, whole, part, tp)


def final_kernel(*refs, order, columns):
    out = refs[-1]
    sp, fs, n_fs = lax.axis_index("sp"), lax.axis_index("fs"), lax.axis_size("fs")
    quarter = out.shape[0]
    for k, places in enumerate(order):
        keep, met, back = refs[3 * k : 3 * k + 3]
        if places is None:
            out[...] = (keep[...].astype(F32) + met[0:quarter].astype(F32) + back[...].astype(F32)).astype(BF16)
            continue
        for j, (c, d) in enumerate(places):
            twin = places.index((c, d ^ 1))
            lanes = slice(j * columns, (j + 1) * columns)
            other = slice(twin * columns, (twin + 1) * columns)
            value = keep[:, lanes].astype(F32) + met[0:quarter, lanes].astype(F32) + back[:, other].astype(F32)
            spot = ((sp ^ d) * n_fs + (fs ^ c)) * columns
            out[:, pl.ds(pl.multiple_of(spot, columns), columns)] = value.astype(BF16)


def per_device(
    tokens,
    norm_gain,
    query_weight,
    forget_weight,
    value_weight,
    outgate_weight,
    pool_in_weight,
    forget_room,
    decay_shift,
    head_gain,
    start_state,
    pool_map,
    pool_scale,
    out_rec_weight,
    out_pool_weight,
):
    n_sp, n_fs = lax.axis_size("sp"), lax.axis_size("fs")
    pair = lax.axis_index("sp") // PAIR
    model = norm_gain.shape[0]
    rows = query_weight.shape[0]
    columns = query_weight.shape[1] // PAIR
    heads = columns // HEAD
    length = tokens.shape[1] * PAIR
    blocks = length // BLOCK
    mine = tokens[0]
    mine_other = swapped(mine, "tp", 1)
    pack_out = [((rows, 5 * columns), BF16)] * 2
    mix_same, mix_other = call(
        pack_kernel,
        pack_out,
        forget_weight,
        value_weight,
        query_weight,
        outgate_weight,
        pool_in_weight,
        scratch=[pltpu.SemaphoreType.DMA((2, 5))],
        outside=range(5),
        room=62,
    )
    line_a = along_line(mix_same, mix_other)
    pack_out = [((out_rec_weight.shape[1], 2 * columns), BF16)] * 2
    out_same, out_other = call(
        pack_rows_kernel,
        pack_out,
        out_rec_weight,
        out_pool_weight,
        scratch=[pltpu.VMEM((2,) + out_rec_weight.shape, BF16), pltpu.SemaphoreType.DMA((2,))],
        outside=range(2),
        room=62,
    )
    half = ((tokens.shape[1], tokens.shape[2]), BF16)
    tail = ((WIDEST, tokens.shape[2]), BF16)
    normed_own, normed_other, ends = call(norm_kernel, [half, half, tail], mine, mine_other, norm_gain[None])
    (before,) = call(merge_kernel, [tail], passed_on(ends, "sp", 1, 1, PAIR), passed_on(ends, "sp", 2, 1, PAIR))
    before_other = swapped(before, "tp", 1)
    near = swapped(normed_own, "sp", 1)
    shift_mine = decay_shift[0].T
    shift_near = swapped(shift_mine, "sp", 1)
    line_c = along_line(out_same, out_other)
    cut = (n_sp + 2) // 2
    fine = [[0], [1], list(range(2, cut)), list(range(cut, n_sp))]
    mix_pieces = over_plane(line_a, fine, "xyyx")
    first_shards, first_where = split([p for p in mix_pieces if p[2][0] < PAIR])
    mix_shards, mix_where = split([p for p in mix_pieces if p[2][0] >= PAIR])
    out_pieces = over_plane(line_c, [[0], list(range(1, n_sp))], "yy")
    near_other = swapped(near, "tp", 1)
    wide = PAIR * n_fs * rows
    normed, earlier = call(
        functools.partial(first_kernel, where=first_where, rows=rows),
        [((length + WIDEST, model), BF16), ((length + WIDEST, 5 * columns), F32)],
        normed_own,
        normed_other,
        near,
        near_other,
        before,
        before_other,
        *first_shards,
        scratch=[pltpu.VMEM((wide, 5 * columns), BF16)],
    )
    value, keyed, within, states, fades, leaving, opening, total, last = call(
        functools.partial(mix_kernel, where=mix_where, rows=rows),
        [
            ((length, columns), BF16),
            ((length, columns), F32),
            ((length, columns), F32),
            ((blocks, heads, HEAD, HEAD), F32),
            ((blocks, heads, HEAD), F32),
            ((heads, HEAD, HEAD), BF16),
            ((heads, HEAD, HEAD), F32),
            ((heads, 1, HEAD), F32),
            ((heads, HEAD, HEAD), F32),
        ],
        normed,
        earlier,
        forget_room[None],
        shift_mine,
        shift_near,
        start_state[0],
        *mix_shards,
        scratch=[
            pltpu.VMEM((model - wide, 2 * columns), BF16),
            pltpu.VMEM((8, length), F32),
            pltpu.VMEM((heads, HEAD, HEAD), F32),
            pltpu.SemaphoreType.DMA(()),
        ],
        outside=(5,),
        room=16,
    )
    arrived = passed_on(leaving, "sp", PAIR)

    def handoff(turn, arrived):
        onward = (total * arrived.astype(F32) + last).astype(BF16)
        onward = jnp.where(pair == 0, leaving, onward)
        return passed_on(onward, "sp", PAIR)

    if n_sp // PAIR > 2:
        arrived = lax.fori_loop(0, n_sp // PAIR - 2, handoff, arrived)
    inside, reach, gate, pool, border = call(
        functools.partial(inside_kernel, where=mix_where, rows=rows),
        [
            ((length, columns), F32),
            ((length, columns), BF16),
            ((length, columns), BF16),
            ((length, columns), BF16),
            ((WIDEST, columns), BF16),
        ],
        normed,
        earlier,
        value,
        keyed,
        within,
        *mix_shards,
        scratch=[pltpu.VMEM((model - wide, 3 * columns), BF16)],
    )
    (joined,) = call(
        join_kernel,
        [((length, 2 * columns), BF16)],
        inside,
        reach,
        states,
        fades,
        opening,
        arrived,
        gate,
        pool,
        head_gain[None],
        border,
        pool_map,
        pool_scale[None],
        scratch=[pltpu.VMEM((WIDEST + length, columns), F32)],
    )
    quarter = length // (PAIR * 2)
    out_rows = out_rec_weight.shape[1]
    if out_rows % 128:
        sets = [out_pieces]
    else:
        sets = [[p for p in out_pieces if p[1] in near_by] for near_by in ((0, 1), (2,), (3,))]
    shares, order = [], []
    for pieces in sets:
        shards, where = split(pieces)
        sort = (where, out_rows) if out_rows % 128 else None
        wide = sum(shard.shape[0] for shard in shards)
        send, whole = call(
            functools.partial(send_kernel, count=len(shards), sort=sort),
            [((2 * quarter, wide), BF16), ((wide, 2 * columns), BF16)],
            joined,
            *shards,
        )
        keep, far = call(keep_kernel, [((quarter, wide), BF16)] * 2, joined, whole)
        met = swapped(send, "tp", 1)
        owed = (far.astype(F32) + met[quarter:].astype(F32)).astype(BF16)
        shares += [keep, met, swapped(owed, "sp", 1)]
        order.append(None if sort else tuple((c, d) for c, group in where for d in group))
    (mixed,) = call(
        functools.partial(final_kernel, order=tuple(order), columns=out_rows), [((quarter, model), BF16)], *shares
    )
    return mixed[None]


def solution(mesh):
    return jax.shard_map(
        per_device,
        mesh=mesh,
        in_specs=(
            P("fs", "sp", "tp"),
            P(),
            P(("sp", "fs"), "tp"),
            P(("sp", "fs"), "tp"),
            P(("sp", "fs"), "tp"),
            P(("sp", "fs"), "tp"),
            P(("sp", "fs"), "tp"),
            P("tp"),
            P("fs", "sp", "tp"),
            P(),
            P("fs", "tp", None, None),
            P("tp", None, None),
            P("tp"),
            P("tp", ("sp", "fs")),
            P("tp", ("sp", "fs")),
        ),
        out_specs=P("fs", ("sp", "tp"), None),
        check_vma=False,
    )
```

```python
import functools

import jax
import jax.numpy as jnp
from jax import lax
from jax.experimental import pallas as pl
from jax.experimental.pallas import tpu as pltpu
from jax.sharding import PartitionSpec as P


HEAD = 128
WIDEST = 16
BLOCK = 128
PAIR = 2
EPSILON = 1e-06
F32 = jnp.float32
BF16 = jnp.bfloat16


def dot(a, b, contract):
    return lax.dot_general(a, b, (contract, ((), ())), preferred_element_type=F32)


def swapped(value, axis, distance):
    count = lax.axis_size(axis)
    return lax.ppermute(value, axis, [(i, i ^ distance) for i in range(count)])


def passed_on(value, axis, steps, first=0, stride=1):
    count = lax.axis_size(axis)
    return lax.ppermute(value, axis, [(i, i + steps) for i in range(first, count - steps, stride)])


def call(kernel, outs, *args, scratch=(), outside=(), room=16):
    vmem = pl.BlockSpec(memory_space=pltpu.VMEM)
    anywhere = pl.BlockSpec(memory_space=pltpu.HBM)
    return pl.pallas_call(
        kernel,
        out_shape=[jax.ShapeDtypeStruct(shape, dtype) for shape, dtype in outs],
        in_specs=[anywhere if k in outside else vmem for k in range(len(args))],
        out_specs=[vmem] * len(outs),
        scratch_shapes=list(scratch),
        compiler_params=pltpu.CompilerParams(vmem_limit_bytes=room * 2**20),
    )(*args)


def along_line(same, other):
    return [same] + [swapped(other if d % PAIR else same, "sp", d) for d in range(1, lax.axis_size("sp"))]


def over_plane(arrived, groups, routes):
    pieces = []
    for group, route in zip(groups, routes):
        plane = arrived[group[0]]
        if len(group) > 1:
            shape = (len(group) * plane.shape[0], plane.shape[1])
            (plane,) = call(stack_kernel, [(shape, BF16)], *(arrived[d] for d in group))
        by_x = swapped(plane, "fs", 1)
        by_y = swapped(plane, "fs", 2)
        pieces += [(plane, 0, tuple(group)), (by_x, 1, tuple(group)), (by_y, 2, tuple(group))]
        if route == "x":
            pieces.append((swapped(by_y, "fs", 1), 3, tuple(group)))
        elif route == "y":
            pieces.append((swapped(by_x, "fs", 2), 3, tuple(group)))
        else:
            count = (len(group) + 1) // 2
            cut = by_x.shape[0] // len(group) * count
            pieces.append((swapped(by_x[:cut], "fs", 2), 3, tuple(group[:count])))
            pieces.append((swapped(by_y[cut:], "fs", 1), 3, tuple(group[count:])))
    return pieces


def stack_kernel(*refs):
    pieces, out = refs[:-1], refs[-1]
    rows = pieces[0].shape[0]
    for k, piece in enumerate(pieces):
        out[k * rows : (k + 1) * rows, :] = piece[...]


def split(pieces):
    return [piece[0] for piece in pieces], tuple(piece[1:] for piece in pieces)


def assemble(refs, where, whole, rows, leading=0, first=0):
    sp, fs, n_fs = lax.axis_index("sp"), lax.axis_index("fs"), lax.axis_size("fs")
    for ref, (c, distances) in zip(refs, where):
        for k, d in enumerate(distances):
            block = (d // PAIR - leading) * PAIR * n_fs * rows
            spot = block + (((sp ^ d) % PAIR) * n_fs + (fs ^ c)) * rows
            cut = ref[k * rows : (k + 1) * rows, first : first + whole.shape[1]]
            whole[pl.ds(pl.multiple_of(spot, rows), rows), :] = cut


def projected_by(normed, whole, rows, leading, upto=None):
    pair, wide = lax.axis_index("sp") // PAIR, PAIR * lax.axis_size("fs") * rows
    total = None
    for k in range(whole.shape[0] // wide):
        features = pl.ds(pl.multiple_of((pair ^ (k + leading)) * wide, wide), wide)
        part = dot(normed[0 : upto or normed.shape[0], features], whole[k * wide : (k + 1) * wide, :], ((1,), (0,)))
        total = part if total is None else total + part
    return total


def pack_kernel(*refs):
    sources, (same, other), sems = refs[:-3], refs[-3:-1], refs[-1]
    part = lax.axis_index("sp") % PAIR
    columns = sources[0].shape[1] // PAIR
    copies = []
    for j, (target, which) in enumerate(((same, part), (other, 1 - part))):
        for k, source in enumerate(sources):
            cut = source.at[:, pl.ds(pl.multiple_of(which * columns, columns), columns)]
            place = target.at[:, k * columns : (k + 1) * columns]
            copies.append(pltpu.make_async_copy(cut, place, sems.at[j, k]))
    for copy in copies:
        copy.start()
    for copy in copies:
        copy.wait()


def pack_rows_kernel(*refs):
    sources, (same, other), held, sems = refs[:-4], refs[-4:-2], refs[-2], refs[-1]
    part = lax.axis_index("sp") % PAIR
    rows = sources[0].shape[0] // PAIR
    copies = []
    for k, source in enumerate(sources):
        copies.append(pltpu.make_async_copy(source, held.at[k], sems.at[k]))
    for copy in copies:
        copy.start()
    for copy in copies:
        copy.wait()
    for target, which in ((same, part), (other, 1 - part)):
        for k in range(len(sources)):
            cut = held[k, pl.ds(pl.multiple_of(which * rows, rows), rows), :]
            target[:, k * rows : (k + 1) * rows] = cut.T


def norm_kernel(mine, mine_other, gain, own_out, other_out, tail_out):
    tp = lax.axis_index("tp")
    width = mine.shape[1]
    here = pl.ds(pl.multiple_of(tp * width, width), width)
    there = pl.ds(pl.multiple_of((1 - tp) * width, width), width)
    a, b = mine[...].astype(F32), mine_other[...].astype(F32)
    total = jnp.sum(a * a, axis=1, keepdims=True) + jnp.sum(b * b, axis=1, keepdims=True)
    scale = lax.rsqrt(total / (2 * width) + EPSILON)
    own = (a * scale * gain[:, here]).astype(BF16)
    own_out[...] = own
    tail_out[...] = own[own.shape[0] - WIDEST :, :]
    other_out[...] = (b * scale * gain[:, there]).astype(BF16)


def merge_kernel(adjacent, second, out):
    out[...] = adjacent[...] + second[...]


def cumulative(ones_below, value):
    high = value.astype(BF16)
    rest = value - high.astype(F32)
    middle = rest.astype(BF16)
    low = (rest - middle.astype(F32)).astype(BF16)
    contract = ((1,), (0,))
    return dot(ones_below, high, contract) + (dot(ones_below, middle, contract) + dot(ones_below, low, contract))


def first_kernel(*refs, where, rows):
    mine, mine_other, near, near_other, before, before_other = refs[:6]
    shards, (normed, sum_out, whole) = refs[6:-3], refs[-3:]
    part, tp = lax.axis_index("sp") % PAIR, lax.axis_index("tp")
    length, width = mine.shape
    here = pl.ds(pl.multiple_of(tp * width, width), width)
    there = pl.ds(pl.multiple_of((1 - tp) * width, width), width)
    for spot, left, right in ((part, mine, mine_other), (1 - part, near, near_other)):
        place = pl.ds(pl.multiple_of(spot * length, length), length)
        normed[place, here] = left[...]
        normed[place, there] = right[...]
    normed[PAIR * length :, here] = before[...]
    normed[PAIR * length :, there] = before_other[...]
    assemble(shards, where, whole, rows)
    sum_out[...] = projected_by(normed, whole, rows, 0)


def mix_kernel(*refs, where, rows):
    normed, earlier, room_whole, shift_mine, shift_near, start = refs[:6]
    shards = refs[6 : 6 + len(where)]
    value_out, keyed_out, within_out, state_out, fade_out, leaving_out, opening_out, total_out, last_out = refs[
        6 + len(where) : 15 + len(where)
    ]
    whole, shift, first, sem = refs[15 + len(where) :]
    part = lax.axis_index("sp") % PAIR
    length, width = keyed_out.shape
    heads = width // HEAD
    fetch = pltpu.make_async_copy(start.at[pl.ds(part * heads, heads)], first, sem)
    fetch.start()
    lines, own = shift_mine.shape
    shift[...] = jnp.zeros_like(shift)
    shift[0:lines, pl.ds(pl.multiple_of(part * own, own), own)] = shift_mine[...]
    shift[0:lines, pl.ds(pl.multiple_of((1 - part) * own, own), own)] = shift_near[...]
    shifts = shift[...].T
    assemble(shards, where, whole, rows, 1)
    projected = earlier[0:length, 0 : 2 * width] + projected_by(normed, whole, rows, 1, length)
    projected = projected.astype(BF16)
    value_out[...] = projected[:, width:]
    room = room_whole[:, pl.ds(pl.multiple_of(part * width, width), width)]
    t = lax.broadcasted_iota(jnp.int32, (BLOCK, BLOCK), 0)
    s = lax.broadcasted_iota(jnp.int32, (BLOCK, BLOCK), 1)
    ones_below = (s <= t).astype(F32).astype(BF16)
    state = [jnp.zeros((HEAD, HEAD), F32) for _ in range(heads)]
    faded = [jnp.zeros((1, HEAD), F32) for _ in range(heads)]
    for n in range(length // BLOCK):
        span = slice(n * BLOCK, (n + 1) * BLOCK)
        logits = projected[span, 0:width].astype(F32)
        value = projected[span, width:]
        keyed = room * (1.0 - jax.nn.sigmoid(logits))
        every = shifts[span, :]
        lags = [
            jnp.where(part == 0, every[:, h : h + 1], every[:, heads + h : heads + h + 1]) for h in range(heads)
        ]
        lag = jnp.concatenate([jnp.broadcast_to(column, (BLOCK, HEAD)) for column in lags], axis=1)
        within = cumulative(ones_below, jnp.log1p(-keyed) + lag)
        keyed_out[span, :] = keyed
        within_out[span, :] = within
        ending = within[BLOCK - 1 : BLOCK]
        late_k = (keyed * jnp.exp(ending - within)).astype(BF16)
        for h in range(heads):
            lanes = slice(h * HEAD, (h + 1) * HEAD)
            state_out[n, h] = state[h]
            fade_out[n, h : h + 1] = jnp.exp(faded[h])
            added = dot(value[:, lanes], late_k[:, lanes], ((0,), (0,)))
            state[h] = jnp.exp(ending[:, lanes]) * state[h] + added
            faded[h] = faded[h] + ending[:, lanes]
    fetch.wait()
    for h in range(heads):
        total = jnp.exp(faded[h])
        opening = first[h].T
        opening_out[h] = opening
        leaving_out[h] = (total * opening + state[h]).astype(BF16)
        last_out[h] = state[h]
        total_out[h] = total


def inside_kernel(*refs, where, rows):
    normed, earlier, value_all, keyed, within_all = refs[:5]
    shards = refs[5 : 5 + len(where)]
    inside_out, reach_out, gate_out, pool_out, border_out, whole = refs[5 + len(where) :]
    length, width = keyed.shape
    assemble(shards, where, whole, rows, 1, 2 * width)
    projected = (earlier[:, 2 * width :] + projected_by(normed, whole, rows, 1)).astype(BF16)
    gate_out[...] = projected[0:length, width : 2 * width]
    pool_out[...] = projected[0:length, 2 * width :]
    border_out[...] = projected[length:, 2 * width :]
    t = lax.broadcasted_iota(jnp.int32, (BLOCK, BLOCK), 0)
    s = lax.broadcasted_iota(jnp.int32, (BLOCK, BLOCK), 1)
    causal = s <= t
    for n in range(length // BLOCK):
        span = slice(n * BLOCK, (n + 1) * BLOCK)
        queries = jax.nn.silu(projected[span, 0:width].astype(F32)) * HEAD ** (-0.5)
        value = value_all[span, :]
        within = within_all[span, :]
        centre = within[BLOCK // 2 - 1 : BLOCK // 2]
        near_q = (queries * jnp.exp(within - centre)).astype(BF16)
        near_k = (keyed[span, :] * jnp.exp(centre - within)).astype(BF16)
        reach_out[span, :] = (queries * jnp.exp(within)).astype(BF16)
        for h in range(width // HEAD):
            lanes = slice(h * HEAD, (h + 1) * HEAD)
            scores = jnp.where(causal, dot(near_q[:, lanes], near_k[:, lanes], ((1,), (1,))), 0.0)
            inside_out[span, lanes] = dot(scores.astype(BF16), value[:, lanes], ((1,), (0,)))


def join_kernel(
    inside, reach, states, fades, opening, arrived, gate, pool, head_gain, border, mappings, scales, joined, extended
):
    length, width = inside.shape
    heads = width // HEAD
    sp, tp = lax.axis_index("sp"), lax.axis_index("tp")
    part, pair = sp % PAIR, sp // PAIR
    for h in range(heads):
        lanes = slice(h * HEAD, (h + 1) * HEAD)
        entering = jnp.where(pair == 0, opening[h], arrived[h].astype(F32))
        for n in range(length // BLOCK):
            span = slice(n * BLOCK, (n + 1) * BLOCK)
            memory = states[n, h] + fades[n, h : h + 1] * entering
            raw = inside[span, lanes] + dot(reach[span, lanes], memory.astype(BF16), ((1,), (1,)))
            level = lax.rsqrt(jnp.mean(raw * raw, axis=1, keepdims=True) + EPSILON)
            gating = jax.nn.silu(gate[span, lanes].astype(F32))
            joined[span, lanes] = (raw * level * head_gain[...] * gating).astype(BF16)
    extended[0:WIDEST, :] = border[...].astype(F32)
    extended[WIDEST:, :] = pool[...].astype(F32)
    sums = extended[...]
    grouping = tp * PAIR + part
    chosen = jnp.zeros((length, width), F32)
    step = 1
    for level in range(4):
        sums = sums[step:, :] + sums[:-step, :]
        step *= 2
        chosen = jnp.where(grouping == level, sums[sums.shape[0] - length :, :], chosen)
    span_length = jnp.left_shift(jnp.int32(2), grouping)
    position = pair * length + lax.broadcasted_iota(jnp.int32, (length, 1), 0)
    amount = jnp.minimum(position + 1, span_length).astype(F32)
    pooled = (chosen / amount - extended[WIDEST:, :]).astype(BF16)
    mapped = dot(pooled, mappings[part], ((1,), (0,)))
    scale = scales[:, pl.ds(pl.multiple_of(part * width, width), width)]
    joined[:, width:] = (mapped * scale).astype(BF16)


def rows_owed(joined, whole, owner_part, owner_tp):
    quarter = joined.shape[0] // (PAIR * 2)
    rows = pl.ds(pl.multiple_of((owner_part * 2 + owner_tp) * quarter, quarter), quarter)
    return dot(joined[rows, :], whole[...], ((1,), (1,))).astype(BF16)


def send_kernel(*refs, count, sort):
    joined, shards = refs[0], refs[1 : 1 + count]
    send_out, whole = refs[1 + count :]
    part, tp = lax.axis_index("sp") % PAIR, lax.axis_index("tp")
    if sort is None:
        spot = 0
        for shard in shards:
            whole[spot : spot + shard.shape[0], :] = shard[...]
            spot += shard.shape[0]
    else:
        where, rows = sort
        sp, fs, n_fs = lax.axis_index("sp"), lax.axis_index("fs"), lax.axis_size("fs")
        for shard, (c, distances) in zip(shards, where):
            for k, d in enumerate(distances):
                spot = ((sp ^ d) * n_fs + (fs ^ c)) * rows
                whole[pl.ds(pl.multiple_of(spot, rows), rows), :] = shard[k * rows : (k + 1) * rows, :]
    quarter = send_out.shape[0] // 2
    send_out[0:quarter, :] = rows_owed(joined, whole, part, 1 - tp)
    send_out[quarter:, :] = rows_owed(joined, whole, 1 - part, 1 - tp)


def keep_kernel(joined, whole, keep_out, far_out):
    part, tp = lax.axis_index("sp") % PAIR, lax.axis_index("tp")
    far_out[...] = rows_owed(joined, whole, 1 - part, tp)
    keep_out[...] = rows_owed(joined, whole, part, tp)


def final_kernel(*refs, order, columns):
    out = refs[-1]
    sp, fs, n_fs = lax.axis_index("sp"), lax.axis_index("fs"), lax.axis_size("fs")
    quarter = out.shape[0]
    for k, places in enumerate(order):
        keep, met, back = refs[3 * k : 3 * k + 3]
        if places is None:
            out[...] = (keep[...].astype(F32) + met[0:quarter].astype(F32) + back[...].astype(F32)).astype(BF16)
            continue
        for j, (c, d) in enumerate(places):
            twin = places.index((c, d ^ 1))
            lanes = slice(j * columns, (j + 1) * columns)
            other = slice(twin * columns, (twin + 1) * columns)
            value = keep[:, lanes].astype(F32) + met[0:quarter, lanes].astype(F32) + back[:, other].astype(F32)
            spot = ((sp ^ d) * n_fs + (fs ^ c)) * columns
            out[:, pl.ds(pl.multiple_of(spot, columns), columns)] = value.astype(BF16)


def per_device(
    tokens,
    norm_gain,
    query_weight,
    forget_weight,
    value_weight,
    outgate_weight,
    pool_in_weight,
    forget_room,
    decay_shift,
    head_gain,
    start_state,
    pool_map,
    pool_scale,
    out_rec_weight,
    out_pool_weight,
):
    n_sp, n_fs = lax.axis_size("sp"), lax.axis_size("fs")
    pair = lax.axis_index("sp") // PAIR
    model = norm_gain.shape[0]
    rows = query_weight.shape[0]
    columns = query_weight.shape[1] // PAIR
    heads = columns // HEAD
    length = tokens.shape[1] * PAIR
    blocks = length // BLOCK
    mine = tokens[0]
    mine_other = swapped(mine, "tp", 1)
    pack_out = [((rows, 5 * columns), BF16)] * 2
    mix_same, mix_other = call(
        pack_kernel,
        pack_out,
        forget_weight,
        value_weight,
        query_weight,
        outgate_weight,
        pool_in_weight,
        scratch=[pltpu.SemaphoreType.DMA((2, 5))],
        outside=range(5),
        room=62,
    )
    line_a = along_line(mix_same, mix_other)
    pack_out = [((out_rec_weight.shape[1], 2 * columns), BF16)] * 2
    out_same, out_other = call(
        pack_rows_kernel,
        pack_out,
        out_rec_weight,
        out_pool_weight,
        scratch=[pltpu.VMEM((2,) + out_rec_weight.shape, BF16), pltpu.SemaphoreType.DMA((2,))],
        outside=range(2),
        room=62,
    )
    half = ((tokens.shape[1], tokens.shape[2]), BF16)
    tail = ((WIDEST, tokens.shape[2]), BF16)
    normed_own, normed_other, ends = call(norm_kernel, [half, half, tail], mine, mine_other, norm_gain[None])
    (before,) = call(merge_kernel, [tail], passed_on(ends, "sp", 1, 1, PAIR), passed_on(ends, "sp", 2, 1, PAIR))
    before_other = swapped(before, "tp", 1)
    near = swapped(normed_own, "sp", 1)
    shift_mine = decay_shift[0].T
    shift_near = swapped(shift_mine, "sp", 1)
    line_c = along_line(out_same, out_other)
    cut = (n_sp + 2) // 2
    fine = [[0], [1], list(range(2, cut)), list(range(cut, n_sp))]
    mix_pieces = over_plane(line_a, fine, "xyyx")
    first_shards, first_where = split([p for p in mix_pieces if p[2][0] < PAIR])
    mix_shards, mix_where = split([p for p in mix_pieces if p[2][0] >= PAIR])
    out_pieces = over_plane(line_c, [[0], list(range(1, n_sp))], "xb")
    near_other = swapped(near, "tp", 1)
    wide = PAIR * n_fs * rows
    normed, earlier = call(
        functools.partial(first_kernel, where=first_where, rows=rows),
        [((length + WIDEST, model), BF16), ((length + WIDEST, 5 * columns), F32)],
        normed_own,
        normed_other,
        near,
        near_other,
        before,
        before_other,
        *first_shards,
        scratch=[pltpu.VMEM((wide, 5 * columns), BF16)],
    )
    value, keyed, within, states, fades, leaving, opening, total, last = call(
        functools.partial(mix_kernel, where=mix_where, rows=rows),
        [
            ((length, columns), BF16),
            ((length, columns), F32),
            ((length, columns), F32),
            ((blocks, heads, HEAD, HEAD), F32),
            ((blocks, heads, HEAD), F32),
            ((heads, HEAD, HEAD), BF16),
            ((heads, HEAD, HEAD), F32),
            ((heads, 1, HEAD), F32),
            ((heads, HEAD, HEAD), F32),
        ],
        normed,
        earlier,
        forget_room[None],
        shift_mine,
        shift_near,
        start_state[0],
        *mix_shards,
        scratch=[
            pltpu.VMEM((model - wide, 2 * columns), BF16),
            pltpu.VMEM((8, length), F32),
            pltpu.VMEM((heads, HEAD, HEAD), F32),
            pltpu.SemaphoreType.DMA(()),
        ],
        outside=(5,),
        room=16,
    )
    arrived = passed_on(leaving, "sp", PAIR)

    def handoff(turn, arrived):
        onward = (total * arrived.astype(F32) + last).astype(BF16)
        onward = jnp.where(pair == 0, leaving, onward)
        return passed_on(onward, "sp", PAIR)

    if n_sp // PAIR > 2:
        arrived = lax.fori_loop(0, n_sp // PAIR - 2, handoff, arrived)
    inside, reach, gate, pool, border = call(
        functools.partial(inside_kernel, where=mix_where, rows=rows),
        [
            ((length, columns), F32),
            ((length, columns), BF16),
            ((length, columns), BF16),
            ((length, columns), BF16),
            ((WIDEST, columns), BF16),
        ],
        normed,
        earlier,
        value,
        keyed,
        within,
        *mix_shards,
        scratch=[pltpu.VMEM((model - wide, 3 * columns), BF16)],
    )
    (joined,) = call(
        join_kernel,
        [((length, 2 * columns), BF16)],
        inside,
        reach,
        states,
        fades,
        opening,
        arrived,
        gate,
        pool,
        head_gain[None],
        border,
        pool_map,
        pool_scale[None],
        scratch=[pltpu.VMEM((WIDEST + length, columns), F32)],
    )
    quarter = length // (PAIR * 2)
    out_rows = out_rec_weight.shape[1]
    if out_rows % 128:
        sets = [out_pieces]
    else:
        sets = [[p for p in out_pieces if p[1] in near_by] for near_by in ((0, 1), (2,), (3,))]
    shares, order = [], []
    for pieces in sets:
        shards, where = split(pieces)
        sort = (where, out_rows) if out_rows % 128 else None
        wide = sum(shard.shape[0] for shard in shards)
        send, whole = call(
            functools.partial(send_kernel, count=len(shards), sort=sort),
            [((2 * quarter, wide), BF16), ((wide, 2 * columns), BF16)],
            joined,
            *shards,
        )
        keep, far = call(keep_kernel, [((quarter, wide), BF16)] * 2, joined, whole)
        met = swapped(send, "tp", 1)
        owed = (far.astype(F32) + met[quarter:].astype(F32)).astype(BF16)
        shares += [keep, met, swapped(owed, "sp", 1)]
        order.append(None if sort else tuple((c, d) for c, group in where for d in group))
    (mixed,) = call(
        functools.partial(final_kernel, order=tuple(order), columns=out_rows), [((quarter, model), BF16)], *shares
    )
    return mixed[None]


def solution(mesh):
    return jax.shard_map(
        per_device,
        mesh=mesh,
        in_specs=(
            P("fs", "sp", "tp"),
            P(),
            P(("sp", "fs"), "tp"),
            P(("sp", "fs"), "tp"),
            P(("sp", "fs"), "tp"),
            P(("sp", "fs"), "tp"),
            P(("sp", "fs"), "tp"),
            P("tp"),
            P("fs", "sp", "tp"),
            P(),
            P("fs", "tp", None, None),
            P("tp", None, None),
            P("tp"),
            P("tp", ("sp", "fs")),
            P("tp", ("sp", "fs")),
        ),
        out_specs=P("fs", ("sp", "tp"), None),
        check_vma=False,
    )
```

```python
import functools

import jax
import jax.numpy as jnp
from jax import lax
from jax.experimental import pallas as pl
from jax.experimental.pallas import tpu as pltpu
from jax.sharding import PartitionSpec as P


HEAD = 128
WIDEST = 16
BLOCK = 128
PAIR = 2
EPSILON = 1e-06
F32 = jnp.float32
BF16 = jnp.bfloat16


def dot(a, b, contract):
    return lax.dot_general(a, b, (contract, ((), ())), preferred_element_type=F32)


def swapped(value, axis, distance):
    count = lax.axis_size(axis)
    return lax.ppermute(value, axis, [(i, i ^ distance) for i in range(count)])


def passed_on(value, axis, steps, first=0, stride=1):
    count = lax.axis_size(axis)
    return lax.ppermute(value, axis, [(i, i + steps) for i in range(first, count - steps, stride)])


def call(kernel, outs, *args, scratch=(), outside=(), room=16):
    vmem = pl.BlockSpec(memory_space=pltpu.VMEM)
    anywhere = pl.BlockSpec(memory_space=pltpu.HBM)
    return pl.pallas_call(
        kernel,
        out_shape=[jax.ShapeDtypeStruct(shape, dtype) for shape, dtype in outs],
        in_specs=[anywhere if k in outside else vmem for k in range(len(args))],
        out_specs=[vmem] * len(outs),
        scratch_shapes=list(scratch),
        compiler_params=pltpu.CompilerParams(vmem_limit_bytes=room * 2**20),
    )(*args)


def along_line(same, other):
    return [same] + [swapped(other if d % PAIR else same, "sp", d) for d in range(1, lax.axis_size("sp"))]


def over_plane(arrived, groups, routes):
    pieces = []
    for group, route in zip(groups, routes):
        plane = arrived[group[0]]
        if len(group) > 1:
            shape = (len(group) * plane.shape[0], plane.shape[1])
            (plane,) = call(stack_kernel, [(shape, BF16)], *(arrived[d] for d in group))
        by_x = swapped(plane, "fs", 1)
        by_y = swapped(plane, "fs", 2)
        pieces += [(plane, 0, tuple(group)), (by_x, 1, tuple(group)), (by_y, 2, tuple(group))]
        if route == "x":
            pieces.append((swapped(by_y, "fs", 1), 3, tuple(group)))
        elif route == "y":
            pieces.append((swapped(by_x, "fs", 2), 3, tuple(group)))
        else:
            count = (len(group) + 1) // 2
            cut = by_x.shape[0] // len(group) * count
            pieces.append((swapped(by_x[:cut], "fs", 2), 3, tuple(group[:count])))
            pieces.append((swapped(by_y[cut:], "fs", 1), 3, tuple(group[count:])))
    return pieces


def stack_kernel(*refs):
    pieces, out = refs[:-1], refs[-1]
    rows = pieces[0].shape[0]
    for k, piece in enumerate(pieces):
        out[k * rows : (k + 1) * rows, :] = piece[...]


def split(pieces):
    return [piece[0] for piece in pieces], tuple(piece[1:] for piece in pieces)


def assemble(refs, where, whole, rows, leading=0, first=0):
    sp, fs, n_fs = lax.axis_index("sp"), lax.axis_index("fs"), lax.axis_size("fs")
    for ref, (c, distances) in zip(refs, where):
        for k, d in enumerate(distances):
            block = (d // PAIR - leading) * PAIR * n_fs * rows
            spot = block + (((sp ^ d) % PAIR) * n_fs + (fs ^ c)) * rows
            cut = ref[k * rows : (k + 1) * rows, first : first + whole.shape[1]]
            whole[pl.ds(pl.multiple_of(spot, rows), rows), :] = cut


def projected_by(normed, whole, rows, leading, upto=None):
    pair, wide = lax.axis_index("sp") // PAIR, PAIR * lax.axis_size("fs") * rows
    total = None
    for k in range(whole.shape[0] // wide):
        features = pl.ds(pl.multiple_of((pair ^ (k + leading)) * wide, wide), wide)
        part = dot(normed[0 : upto or normed.shape[0], features], whole[k * wide : (k + 1) * wide, :], ((1,), (0,)))
        total = part if total is None else total + part
    return total


def pack_kernel(*refs):
    sources, (same, other), sems = refs[:-3], refs[-3:-1], refs[-1]
    part = lax.axis_index("sp") % PAIR
    columns = sources[0].shape[1] // PAIR
    copies = []
    for j, (target, which) in enumerate(((same, part), (other, 1 - part))):
        for k, source in enumerate(sources):
            cut = source.at[:, pl.ds(pl.multiple_of(which * columns, columns), columns)]
            place = target.at[:, k * columns : (k + 1) * columns]
            copies.append(pltpu.make_async_copy(cut, place, sems.at[j, k]))
    for copy in copies:
        copy.start()
    for copy in copies:
        copy.wait()


def pack_rows_kernel(*refs):
    sources, (same, other), held, sems = refs[:-4], refs[-4:-2], refs[-2], refs[-1]
    part = lax.axis_index("sp") % PAIR
    rows = sources[0].shape[0] // PAIR
    copies = []
    for k, source in enumerate(sources):
        copies.append(pltpu.make_async_copy(source, held.at[k], sems.at[k]))
    for copy in copies:
        copy.start()
    for copy in copies:
        copy.wait()
    for target, which in ((same, part), (other, 1 - part)):
        for k in range(len(sources)):
            cut = held[k, pl.ds(pl.multiple_of(which * rows, rows), rows), :]
            target[:, k * rows : (k + 1) * rows] = cut.T


def norm_kernel(mine, mine_other, gain, own_out, other_out, tail_out):
    tp = lax.axis_index("tp")
    width = mine.shape[1]
    here = pl.ds(pl.multiple_of(tp * width, width), width)
    there = pl.ds(pl.multiple_of((1 - tp) * width, width), width)
    a, b = mine[...].astype(F32), mine_other[...].astype(F32)
    total = jnp.sum(a * a, axis=1, keepdims=True) + jnp.sum(b * b, axis=1, keepdims=True)
    scale = lax.rsqrt(total / (2 * width) + EPSILON)
    own = (a * scale * gain[:, here]).astype(BF16)
    own_out[...] = own
    tail_out[...] = own[own.shape[0] - WIDEST :, :]
    other_out[...] = (b * scale * gain[:, there]).astype(BF16)


def merge_kernel(adjacent, second, out):
    out[...] = adjacent[...] + second[...]


def cumulative(ones_below, value):
    high = value.astype(BF16)
    rest = value - high.astype(F32)
    middle = rest.astype(BF16)
    low = (rest - middle.astype(F32)).astype(BF16)
    contract = ((1,), (0,))
    return dot(ones_below, high, contract) + (dot(ones_below, middle, contract) + dot(ones_below, low, contract))


def first_kernel(*refs, where, rows):
    mine, mine_other, near, near_other, before, before_other = refs[:6]
    shards, (normed, sum_out, whole) = refs[6:-3], refs[-3:]
    part, tp = lax.axis_index("sp") % PAIR, lax.axis_index("tp")
    length, width = mine.shape
    here = pl.ds(pl.multiple_of(tp * width, width), width)
    there = pl.ds(pl.multiple_of((1 - tp) * width, width), width)
    for spot, left, right in ((part, mine, mine_other), (1 - part, near, near_other)):
        place = pl.ds(pl.multiple_of(spot * length, length), length)
        normed[place, here] = left[...]
        normed[place, there] = right[...]
    normed[PAIR * length :, here] = before[...]
    normed[PAIR * length :, there] = before_other[...]
    assemble(shards, where, whole, rows)
    sum_out[...] = projected_by(normed, whole, rows, 0)


def mix_kernel(*refs, where, rows):
    normed, earlier, room_whole, shift_mine, shift_near, start = refs[:6]
    shards = refs[6 : 6 + len(where)]
    value_out, keyed_out, within_out, state_out, fade_out, leaving_out, opening_out, total_out, last_out = refs[
        6 + len(where) : 15 + len(where)
    ]
    whole, shift, first, sem = refs[15 + len(where) :]
    part = lax.axis_index("sp") % PAIR
    length, width = keyed_out.shape
    heads = width // HEAD
    fetch = pltpu.make_async_copy(start.at[pl.ds(part * heads, heads)], first, sem)
    fetch.start()
    lines, own = shift_mine.shape
    shift[...] = jnp.zeros_like(shift)
    shift[0:lines, pl.ds(pl.multiple_of(part * own, own), own)] = shift_mine[...]
    shift[0:lines, pl.ds(pl.multiple_of((1 - part) * own, own), own)] = shift_near[...]
    shifts = shift[...].T
    assemble(shards, where, whole, rows, 1)
    projected = earlier[0:length, 0 : 2 * width] + projected_by(normed, whole, rows, 1, length)
    projected = projected.astype(BF16)
    value_out[...] = projected[:, width:]
    room = room_whole[:, pl.ds(pl.multiple_of(part * width, width), width)]
    t = lax.broadcasted_iota(jnp.int32, (BLOCK, BLOCK), 0)
    s = lax.broadcasted_iota(jnp.int32, (BLOCK, BLOCK), 1)
    ones_below = (s <= t).astype(F32).astype(BF16)
    state = [jnp.zeros((HEAD, HEAD), F32) for _ in range(heads)]
    faded = [jnp.zeros((1, HEAD), F32) for _ in range(heads)]
    for n in range(length // BLOCK):
        span = slice(n * BLOCK, (n + 1) * BLOCK)
        logits = projected[span, 0:width].astype(F32)
        value = projected[span, width:]
        keyed = room * (1.0 - jax.nn.sigmoid(logits))
        every = shifts[span, :]
        lags = [
            jnp.where(part == 0, every[:, h : h + 1], every[:, heads + h : heads + h + 1]) for h in range(heads)
        ]
        lag = jnp.concatenate([jnp.broadcast_to(column, (BLOCK, HEAD)) for column in lags], axis=1)
        within = cumulative(ones_below, jnp.log1p(-keyed) + lag)
        keyed_out[span, :] = keyed
        within_out[span, :] = within
        ending = within[BLOCK - 1 : BLOCK]
        late_k = (keyed * jnp.exp(ending - within)).astype(BF16)
        for h in range(heads):
            lanes = slice(h * HEAD, (h + 1) * HEAD)
            state_out[n, h] = state[h]
            fade_out[n, h : h + 1] = jnp.exp(faded[h])
            added = dot(value[:, lanes], late_k[:, lanes], ((0,), (0,)))
            state[h] = jnp.exp(ending[:, lanes]) * state[h] + added
            faded[h] = faded[h] + ending[:, lanes]
    fetch.wait()
    for h in range(heads):
        total = jnp.exp(faded[h])
        opening = first[h].T
        opening_out[h] = opening
        leaving_out[h] = (total * opening + state[h]).astype(BF16)
        last_out[h] = state[h]
        total_out[h] = total


def inside_kernel(*refs, where, rows):
    normed, earlier, value_all, keyed, within_all = refs[:5]
    shards = refs[5 : 5 + len(where)]
    inside_out, reach_out, gate_out, pool_out, border_out, whole = refs[5 + len(where) :]
    length, width = keyed.shape
    assemble(shards, where, whole, rows, 1, 2 * width)
    projected = (earlier[:, 2 * width :] + projected_by(normed, whole, rows, 1)).astype(BF16)
    gate_out[...] = projected[0:length, width : 2 * width]
    pool_out[...] = projected[0:length, 2 * width :]
    border_out[...] = projected[length:, 2 * width :]
    t = lax.broadcasted_iota(jnp.int32, (BLOCK, BLOCK), 0)
    s = lax.broadcasted_iota(jnp.int32, (BLOCK, BLOCK), 1)
    causal = s <= t
    for n in range(length // BLOCK):
        span = slice(n * BLOCK, (n + 1) * BLOCK)
        queries = jax.nn.silu(projected[span, 0:width].astype(F32)) * HEAD ** (-0.5)
        value = value_all[span, :]
        within = within_all[span, :]
        centre = within[BLOCK // 2 - 1 : BLOCK // 2]
        near_q = (queries * jnp.exp(within - centre)).astype(BF16)
        near_k = (keyed[span, :] * jnp.exp(centre - within)).astype(BF16)
        reach_out[span, :] = (queries * jnp.exp(within)).astype(BF16)
        for h in range(width // HEAD):
            lanes = slice(h * HEAD, (h + 1) * HEAD)
            scores = jnp.where(causal, dot(near_q[:, lanes], near_k[:, lanes], ((1,), (1,))), 0.0)
            inside_out[span, lanes] = dot(scores.astype(BF16), value[:, lanes], ((1,), (0,)))


def join_kernel(
    inside, reach, states, fades, opening, arrived, gate, pool, head_gain, border, mappings, scales, joined, extended
):
    length, width = inside.shape
    heads = width // HEAD
    sp, tp = lax.axis_index("sp"), lax.axis_index("tp")
    part, pair = sp % PAIR, sp // PAIR
    for h in range(heads):
        lanes = slice(h * HEAD, (h + 1) * HEAD)
        entering = jnp.where(pair == 0, opening[h], arrived[h].astype(F32))
        for n in range(length // BLOCK):
            span = slice(n * BLOCK, (n + 1) * BLOCK)
            memory = states[n, h] + fades[n, h : h + 1] * entering
            raw = inside[span, lanes] + dot(reach[span, lanes], memory.astype(BF16), ((1,), (1,)))
            level = lax.rsqrt(jnp.mean(raw * raw, axis=1, keepdims=True) + EPSILON)
            gating = jax.nn.silu(gate[span, lanes].astype(F32))
            joined[span, lanes] = (raw * level * head_gain[...] * gating).astype(BF16)
    extended[0:WIDEST, :] = border[...].astype(F32)
    extended[WIDEST:, :] = pool[...].astype(F32)
    sums = extended[...]
    grouping = tp * PAIR + part
    chosen = jnp.zeros((length, width), F32)
    step = 1
    for level in range(4):
        sums = sums[step:, :] + sums[:-step, :]
        step *= 2
        chosen = jnp.where(grouping == level, sums[sums.shape[0] - length :, :], chosen)
    span_length = jnp.left_shift(jnp.int32(2), grouping)
    position = pair * length + lax.broadcasted_iota(jnp.int32, (length, 1), 0)
    amount = jnp.minimum(position + 1, span_length).astype(F32)
    pooled = (chosen / amount - extended[WIDEST:, :]).astype(BF16)
    mapped = dot(pooled, mappings[part], ((1,), (0,)))
    scale = scales[:, pl.ds(pl.multiple_of(part * width, width), width)]
    joined[:, width:] = (mapped * scale).astype(BF16)


def rows_owed(joined, whole, owner_part, owner_tp):
    quarter = joined.shape[0] // (PAIR * 2)
    rows = pl.ds(pl.multiple_of((owner_part * 2 + owner_tp) * quarter, quarter), quarter)
    return dot(joined[rows, :], whole[...], ((1,), (1,))).astype(BF16)


def send_kernel(*refs, count, sort):
    joined, shards = refs[0], refs[1 : 1 + count]
    send_out, whole = refs[1 + count :]
    part, tp = lax.axis_index("sp") % PAIR, lax.axis_index("tp")
    if sort is None:
        spot = 0
        for shard in shards:
            whole[spot : spot + shard.shape[0], :] = shard[...]
            spot += shard.shape[0]
    else:
        where, rows = sort
        sp, fs, n_fs = lax.axis_index("sp"), lax.axis_index("fs"), lax.axis_size("fs")
        for shard, (c, distances) in zip(shards, where):
            for k, d in enumerate(distances):
                spot = ((sp ^ d) * n_fs + (fs ^ c)) * rows
                whole[pl.ds(pl.multiple_of(spot, rows), rows), :] = shard[k * rows : (k + 1) * rows, :]
    quarter = send_out.shape[0] // 2
    send_out[0:quarter, :] = rows_owed(joined, whole, part, 1 - tp)
    send_out[quarter:, :] = rows_owed(joined, whole, 1 - part, 1 - tp)


def far_kernel(joined, whole, far_out):
    part, tp = lax.axis_index("sp") % PAIR, lax.axis_index("tp")
    far_out[...] = rows_owed(joined, whole, 1 - part, tp)


def keep_kernel(joined, whole, keep_out):
    part, tp = lax.axis_index("sp") % PAIR, lax.axis_index("tp")
    keep_out[...] = rows_owed(joined, whole, part, tp)


def final_kernel(*refs, order, columns):
    out = refs[-1]
    sp, fs, n_fs = lax.axis_index("sp"), lax.axis_index("fs"), lax.axis_size("fs")
    quarter = out.shape[0]
    for k, places in enumerate(order):
        keep, met, back = refs[3 * k : 3 * k + 3]
        if places is None:
            out[...] = (keep[...].astype(F32) + met[0:quarter].astype(F32) + back[...].astype(F32)).astype(BF16)
            continue
        for j, (c, d) in enumerate(places):
            twin = places.index((c, d ^ 1))
            lanes = slice(j * columns, (j + 1) * columns)
            other = slice(twin * columns, (twin + 1) * columns)
            value = keep[:, lanes].astype(F32) + met[0:quarter, lanes].astype(F32) + back[:, other].astype(F32)
            spot = ((sp ^ d) * n_fs + (fs ^ c)) * columns
            out[:, pl.ds(pl.multiple_of(spot, columns), columns)] = value.astype(BF16)


def per_device(
    tokens,
    norm_gain,
    query_weight,
    forget_weight,
    value_weight,
    outgate_weight,
    pool_in_weight,
    forget_room,
    decay_shift,
    head_gain,
    start_state,
    pool_map,
    pool_scale,
    out_rec_weight,
    out_pool_weight,
):
    n_sp, n_fs = lax.axis_size("sp"), lax.axis_size("fs")
    pair = lax.axis_index("sp") // PAIR
    model = norm_gain.shape[0]
    rows = query_weight.shape[0]
    columns = query_weight.shape[1] // PAIR
    heads = columns // HEAD
    length = tokens.shape[1] * PAIR
    blocks = length // BLOCK
    mine = tokens[0]
    mine_other = swapped(mine, "tp", 1)
    pack_out = [((rows, 5 * columns), BF16)] * 2
    mix_same, mix_other = call(
        pack_kernel,
        pack_out,
        forget_weight,
        value_weight,
        query_weight,
        outgate_weight,
        pool_in_weight,
        scratch=[pltpu.SemaphoreType.DMA((2, 5))],
        outside=range(5),
        room=62,
    )
    line_a = along_line(mix_same, mix_other)
    pack_out = [((out_rec_weight.shape[1], 2 * columns), BF16)] * 2
    out_same, out_other = call(
        pack_rows_kernel,
        pack_out,
        out_rec_weight,
        out_pool_weight,
        scratch=[pltpu.VMEM((2,) + out_rec_weight.shape, BF16), pltpu.SemaphoreType.DMA((2,))],
        outside=range(2),
        room=62,
    )
    half = ((tokens.shape[1], tokens.shape[2]), BF16)
    tail = ((WIDEST, tokens.shape[2]), BF16)
    normed_own, normed_other, ends = call(norm_kernel, [half, half, tail], mine, mine_other, norm_gain[None])
    (before,) = call(merge_kernel, [tail], passed_on(ends, "sp", 1, 1, PAIR), passed_on(ends, "sp", 2, 1, PAIR))
    before_other = swapped(before, "tp", 1)
    near = swapped(normed_own, "sp", 1)
    shift_mine = decay_shift[0].T
    shift_near = swapped(shift_mine, "sp", 1)
    line_c = along_line(out_same, out_other)
    cut = (n_sp + 2) // 2
    fine = [[0], [1], list(range(2, cut)), list(range(cut, n_sp))]
    mix_pieces = over_plane(line_a, fine, "xyyx")
    first_shards, first_where = split([p for p in mix_pieces if p[2][0] < PAIR])
    mix_shards, mix_where = split([p for p in mix_pieces if p[2][0] >= PAIR])
    out_pieces = over_plane(line_c, [[0], list(range(1, n_sp))], "xb")
    near_other = swapped(near, "tp", 1)
    wide = PAIR * n_fs * rows
    normed, earlier = call(
        functools.partial(first_kernel, where=first_where, rows=rows),
        [((length + WIDEST, model), BF16), ((length + WIDEST, 5 * columns), F32)],
        normed_own,
        normed_other,
        near,
        near_other,
        before,
        before_other,
        *first_shards,
        scratch=[pltpu.VMEM((wide, 5 * columns), BF16)],
    )
    value, keyed, within, states, fades, leaving, opening, total, last = call(
        functools.partial(mix_kernel, where=mix_where, rows=rows),
        [
            ((length, columns), BF16),
            ((length, columns), F32),
            ((length, columns), F32),
            ((blocks, heads, HEAD, HEAD), F32),
            ((blocks, heads, HEAD), F32),
            ((heads, HEAD, HEAD), BF16),
            ((heads, HEAD, HEAD), F32),
            ((heads, 1, HEAD), F32),
            ((heads, HEAD, HEAD), F32),
        ],
        normed,
        earlier,
        forget_room[None],
        shift_mine,
        shift_near,
        start_state[0],
        *mix_shards,
        scratch=[
            pltpu.VMEM((model - wide, 2 * columns), BF16),
            pltpu.VMEM((8, length), F32),
            pltpu.VMEM((heads, HEAD, HEAD), F32),
            pltpu.SemaphoreType.DMA(()),
        ],
        outside=(5,),
        room=16,
    )
    arrived = passed_on(leaving, "sp", PAIR)

    def handoff(turn, arrived):
        onward = (total * arrived.astype(F32) + last).astype(BF16)
        onward = jnp.where(pair == 0, leaving, onward)
        return passed_on(onward, "sp", PAIR)

    if n_sp // PAIR > 2:
        arrived = lax.fori_loop(0, n_sp // PAIR - 2, handoff, arrived)
    inside, reach, gate, pool, border = call(
        functools.partial(inside_kernel, where=mix_where, rows=rows),
        [
            ((length, columns), F32),
            ((length, columns), BF16),
            ((length, columns), BF16),
            ((length, columns), BF16),
            ((WIDEST, columns), BF16),
        ],
        normed,
        earlier,
        value,
        keyed,
        within,
        *mix_shards,
        scratch=[pltpu.VMEM((model - wide, 3 * columns), BF16)],
    )
    (joined,) = call(
        join_kernel,
        [((length, 2 * columns), BF16)],
        inside,
        reach,
        states,
        fades,
        opening,
        arrived,
        gate,
        pool,
        head_gain[None],
        border,
        pool_map,
        pool_scale[None],
        scratch=[pltpu.VMEM((WIDEST + length, columns), F32)],
    )
    quarter = length // (PAIR * 2)
    out_rows = out_rec_weight.shape[1]
    if out_rows % 128:
        sets = [out_pieces]
    else:
        sets = [[p for p in out_pieces if p[1] in near_by] for near_by in ((0, 1), (2,), (3,))]
    shares, order = [], []
    for pieces in sets:
        shards, where = split(pieces)
        sort = (where, out_rows) if out_rows % 128 else None
        wide = sum(shard.shape[0] for shard in shards)
        send, whole = call(
            functools.partial(send_kernel, count=len(shards), sort=sort),
            [((2 * quarter, wide), BF16), ((wide, 2 * columns), BF16)],
            joined,
            *shards,
        )
        (far,) = call(far_kernel, [((quarter, wide), BF16)], joined, whole)
        (keep,) = call(keep_kernel, [((quarter, wide), BF16)], joined, whole)
        met = swapped(send, "tp", 1)
        owed = (far.astype(F32) + met[quarter:].astype(F32)).astype(BF16)
        shares += [keep, met, swapped(owed, "sp", 1)]
        order.append(None if sort else tuple((c, d) for c, group in where for d in group))
    (mixed,) = call(
        functools.partial(final_kernel, order=tuple(order), columns=out_rows), [((quarter, model), BF16)], *shares
    )
    return mixed[None]


def solution(mesh):
    return jax.shard_map(
        per_device,
        mesh=mesh,
        in_specs=(
            P("fs", "sp", "tp"),
            P(),
            P(("sp", "fs"), "tp"),
            P(("sp", "fs"), "tp"),
            P(("sp", "fs"), "tp"),
            P(("sp", "fs"), "tp"),
            P(("sp", "fs"), "tp"),
            P("tp"),
            P("fs", "sp", "tp"),
            P(),
            P("fs", "tp", None, None),
            P("tp", None, None),
            P("tp"),
            P("tp", ("sp", "fs")),
            P("tp", ("sp", "fs")),
        ),
        out_specs=P("fs", ("sp", "tp"), None),
        check_vma=False,
    )
```
